32 devices in a mesh: ep: 4 (over y, x), tp: 8 (over z, core).
Axes of the slice: x: 2, y: 2, z: 4, core: 2. Of those that a mesh axis runs over, the one named last changes fastest.
Arguments:
- tokens: bfloat16 [512, 2048], P('ep'), may hold values from -32 to 32
- routes: int32 [512, 2], P('ep'), may hold values from 0 to 3, all different within a row; in each aligned block of 128 rows (0 to 127, 128 to 255, ...) at most 96 rows name the same one
- gates: float32 [512, 2], P('ep'), may hold values from 0.05 to 0.6
- cotangent: bfloat16 [512, 2048], P('ep'), may hold values from -6 to 6
- w_glu: bfloat16 [4, 2048, 1024], P('ep', None, 'tp'), may hold values from -0.125 to 0.125
- w_lin: bfloat16 [4, 2048, 1024], P('ep', None, 'tp'), may hold values from -0.125 to 0.125
- w_down: bfloat16 [4, 1024, 2048], P('ep', 'tp'), may hold values from -0.1875 to 0.1875
Outputs:
- d_tokens: bfloat16 [512, 2048], P('ep', 'tp')
- d_gates: float32 [512, 2], P('ep')
- glu_wgrad: float32 [4, 2048, 1024], P('ep', None, 'tp')
- lin_wgrad: float32 [4, 2048, 1024], P('ep', None, 'tp')
- down_wgrad: float32 [4, 1024, 2048], P('ep', 'tp')
- glu_norms: float32 [4, 2048], P('ep')
- lin_norms: float32 [4, 2048], P('ep')
- down_norms: float32 [4, 1024], P('ep', 'tp')
The draws below stay inside these ranges and needn't reach their ends.
Inputs may be any that keep to these rules, and one draw needn't show every extreme that they name: `routes`: each row names 2 different experts. Among the 128 tokens of one aligned block no expert is named more than 96 times, and in every draw some expert is named exactly 96 times in some block.
All inputs are finite; a program needn't handle non-finite values.
Results may differ from the reference program's by a relative error of at most 0.024.
Values may be sent and summed in bfloat16 or wider, within the bound.
A program may use at most 64 MiB of HBM per device.

```python
import math
import jax
import jax.numpy as jnp
import numpy as np
from jax import lax

D = 2048
F = 1024
TOP = 2
TOK_DEV = 128
EXPERTS = 4
CAP = 96
TOKENS = 512
N_EP = 4
N_TP = 8


def draw_tokens(key, part):
    first_key, second_key, third_key = jax.random.split(key, 3)
    values = jnp.clip(jax.random.normal(first_key, (TOKENS, D), jnp.float32), -4.0, 4.0)
    return values.astype(jnp.bfloat16)


def steps_of(key, extent, cuts, least, largest):
    loudness = 1.0
    for axis_at, shards_of in cuts:
        steps = jax.random.uniform(jax.random.fold_in(jax.random.fold_in(key, 6), axis_at), (shards_of,), jnp.float32, least / len(cuts), largest / len(cuts))
        loudness = loudness * jnp.repeat(jnp.exp(steps), extent[axis_at] // shards_of).reshape((-1,) + (1,) * (len(extent) - 1 - axis_at))
    return loudness


def routed_block(own_key, own, number, rows, number_of, top, reach, slope):
    sequence = jax.random.permutation(own_key, number_of)
    packed, common = portions_of(number_of, rows * top, reach, slope, True), portions_of(number_of, rows * top, reach, slope, False)
    places = jnp.arange(number_of)

    def named(sizes, turn):
        used = int((sizes > 0).sum())
        fixed = max(1, used // 4)
        shifted = fixed + (places - fixed + turn * (used - fixed)) % max(1, number_of - fixed)
        return jnp.zeros((number_of,), jnp.int32).at[sequence[jnp.where(places < fixed, places, shifted)]].set(jnp.asarray(sizes, jnp.int32))

    sizes = jnp.where(number % 4 == 0, named(packed, number // 4), named(common, number - number // 4 - 1))
    mixed = jax.random.permutation(jax.random.fold_in(own, 3), number_of)
    source_of, sink = mixed[0:number_of // 2 * 2:2], mixed[1:number_of // 2 * 2:2]
    margin = jnp.minimum(sizes[source_of] - 1, reach - sizes[sink]) // 2
    margin = jnp.where((source_of == sequence[0]) | (sink == sequence[0]) | (sizes[sink] == 0), 0, jnp.maximum(margin, 0))
    shifted = jax.random.randint(jax.random.fold_in(own, 4), (number_of // 2,), 0, 1 << 20) % (margin + 1)
    sizes = sizes.at[source_of].add(-shifted).at[sink].add(shifted)
    members = jnp.searchsorted(jnp.cumsum(sizes), jnp.arange(rows * top), side="right").astype(jnp.int32)
    listing = members.reshape(top, rows).T
    listing = listing[jax.random.permutation(jax.random.fold_in(own, 1), rows)]
    turn = jax.random.randint(jax.random.fold_in(own, 2), (rows, 1), 0, top)
    return jnp.take_along_axis(listing, (jnp.arange(top)[None, :] + turn) % top, axis=1)


def portions_of(count, total, most, lean, full):
    portions = [(1 << 20) // math.isqrt(grade ** lean) + 1 for grade in range(1, count + 1)]
    largest = most if full else min(most, max(-(-total // count), total * portions[0] // sum(portions)))
    least = 1 if total - largest >= count - 1 else 0
    counts, spare = [largest] + [least] * (count - 1), total - largest - least * (count - 1)
    while spare > 0:
        candidates = [i for i in range(1, count) if counts[i] < largest] or [i for i in range(1, count) if counts[i] < most]
        mass, left = sum([portions[i] for i in candidates]), spare
        for i in candidates:
            addition = min(most - counts[i], max(1, left * portions[i] // mass), spare)
            counts[i] = counts[i] + addition
            spare = spare - addition
    return np.array(counts)


def normal_values(own_key, dims, deviation, bound, shards=(), kind=jnp.bfloat16):
    array = deviation * jax.random.normal(own_key, dims, jnp.float32)
    if shards:
        array = array * steps_of(own_key, dims, shards, -0.22, 0.18)
    return jnp.clip(array, -bound, bound).astype(kind)


def setup_inputs(seed: int = 0) -> dict:
    streams_of = jax.random.split(jax.random.key(seed), 8)
    tokens = draw_tokens(jax.random.fold_in(streams_of[7], 71), 0)
    routes_keys = jax.random.split(jax.random.fold_in(streams_of[1], 1), TOKENS // TOK_DEV)
    routes_turns = jax.random.permutation(jax.random.fold_in(streams_of[1], 3), TOKENS // TOK_DEV)
    routes = jax.vmap(lambda own, number: routed_block(jax.random.fold_in(streams_of[1], 2), own, number, TOK_DEV, EXPERTS, TOP, CAP, 2))(routes_keys, routes_turns).reshape((TOKENS, TOP))
    gates = jnp.clip(jnp.exp(math.log(0.6) - 2.4849067 * jax.random.uniform(streams_of[2], (TOKENS, TOP), jnp.float32) ** steps_of(streams_of[2], (TOKENS, TOP), ((0, 4),), -0.2, 0.2)), 0.05, 0.6)
    cotangent = normal_values(streams_of[3], (TOKENS, D), 1.0, 6.0, ((0, 4),))
    w_glu = normal_values(streams_of[4], (EXPERTS, D, F), D ** -0.5, 0.125, ((0, 4), (2, 8)))
    w_lin = normal_values(streams_of[5], (EXPERTS, D, F), D ** -0.5, 0.125, ((0, 4), (2, 8)))
    w_down = normal_values(streams_of[6], (EXPERTS, F, D), F ** -0.5, 0.1875, ((0, 4), (1, 8)))
    return {"tokens": tokens, "routes": routes, "gates": gates, "cotangent": cotangent, "w_glu": w_glu, "w_lin": w_lin, "w_down": w_down}


clamp_limit = 7.0
sigmoid_scale = 1.702


def slot_rank(pair_expert, all_experts):
    onehot = (pair_expert[:, None] == jnp.arange(all_experts, dtype=jnp.int32)[None, :]).astype(jnp.int32)
    return (jnp.sum(jnp.cumsum(onehot, axis=0) * onehot, axis=1) - 1).astype(jnp.int32)


def clamp_backward(glu_pre, lin_pre, back_proj, gate_col):
    glu_clip = jnp.minimum(glu_pre, clamp_limit)
    lin_clip = jnp.clip(lin_pre, -clamp_limit, clamp_limit)
    sig_val = jax.nn.sigmoid(sigmoid_scale * glu_clip)
    glu_act = glu_clip * sig_val
    hidden = glu_act * (lin_clip + 1.0)
    hid_grad = gate_col * back_proj
    act_slope = sig_val + sigmoid_scale * glu_clip * sig_val * (1.0 - sig_val)
    glu_grad = jnp.where(glu_pre < clamp_limit, hid_grad * (lin_clip + 1.0) * act_slope, 0.0)
    lin_grad = jnp.where(jnp.abs(lin_pre) < clamp_limit, hid_grad * glu_act, 0.0)
    return hidden, glu_grad.astype(jnp.bfloat16), lin_grad.astype(jnp.bfloat16)


def expert_grads(tok_rows, cot_rows, gate_col, glu_w, lin_w, down_w):
    glu_pre = jnp.dot(tok_rows, glu_w, preferred_element_type=jnp.float32)
    lin_pre = jnp.dot(tok_rows, lin_w, preferred_element_type=jnp.float32)
    back_proj = jnp.dot(cot_rows, down_w.T, preferred_element_type=jnp.float32)
    hidden, glu_bf, lin_bf = clamp_backward(glu_pre, lin_pre, back_proj, gate_col)
    gate_part = jnp.sum(back_proj * hidden, axis=1)
    hidden_gated = (gate_col * hidden).astype(jnp.bfloat16)
    down_wgrad = jnp.dot(hidden_gated.T, cot_rows, preferred_element_type=jnp.float32)
    glu_wgrad = jnp.dot(tok_rows.T, glu_bf, preferred_element_type=jnp.float32)
    lin_wgrad = jnp.dot(tok_rows.T, lin_bf, preferred_element_type=jnp.float32)
    return gate_part, glu_bf, lin_bf, glu_wgrad, lin_wgrad, down_wgrad


def rank_block(block_row):
    return slot_rank(block_row, EXPERTS)


def reference(tokens, routes, gates, cotangent, w_glu, w_lin, w_down):
    pair_count = TOK_DEV * TOP
    slot_total = N_EP * CAP
    block_width = F // N_TP
    block_experts = routes.reshape(N_EP, pair_count)
    ranks = jax.vmap(rank_block)(block_experts)
    sources = jnp.arange(N_EP, dtype=jnp.int32)[:, None] * CAP
    slot_index = (block_experts * slot_total + sources + ranks).reshape(-1).astype(jnp.int32)
    slot_pair = jnp.full((EXPERTS * slot_total,), TOKENS * TOP, jnp.int32).at[slot_index].set(
        jnp.arange(TOKENS * TOP, dtype=jnp.int32)).reshape(EXPERTS, slot_total)
    slot_token = (slot_pair // TOP).astype(jnp.int32)
    tok_ext = jnp.concatenate([tokens, jnp.zeros((1, D), jnp.bfloat16)], axis=0)
    cot_ext = jnp.concatenate([cotangent, jnp.zeros((1, D), jnp.bfloat16)], axis=0)
    gate_ext = jnp.concatenate([gates.reshape(-1), jnp.zeros((1,), jnp.float32)])

    def one_expert(inputs):
        token_ids, pair_ids, glu_w, lin_w, down_w = inputs
        tok_rows = tok_ext[token_ids]
        cot_rows = cot_ext[token_ids]
        gate_col = gate_ext[pair_ids][:, None]
        gate_part, glu_bf, lin_bf, glu_wgrad, lin_wgrad, down_wgrad = expert_grads(
            tok_rows, cot_rows, gate_col, glu_w, lin_w, down_w)
        glu_blocks = glu_bf.reshape(slot_total, N_TP, block_width).transpose(1, 0, 2)
        lin_blocks = lin_bf.reshape(slot_total, N_TP, block_width).transpose(1, 0, 2)
        glu_wblocks = glu_w.reshape(D, N_TP, block_width).transpose(1, 0, 2)
        lin_wblocks = lin_w.reshape(D, N_TP, block_width).transpose(1, 0, 2)

        def add_block(total, pieces):
            glu_piece, lin_piece, glu_wpiece, lin_wpiece = pieces
            term = jnp.dot(glu_piece, glu_wpiece.T, preferred_element_type=jnp.float32)
            term = term + jnp.dot(lin_piece, lin_wpiece.T, preferred_element_type=jnp.float32)
            rounded = lax.optimization_barrier(term.astype(jnp.bfloat16))
            return total + rounded.astype(jnp.float32), None

        total, unused = lax.scan(add_block, jnp.zeros((slot_total, D), jnp.float32),
                                 (glu_blocks, lin_blocks, glu_wblocks, lin_wblocks))
        return total.astype(jnp.bfloat16), gate_part, glu_wgrad, lin_wgrad, down_wgrad

    slot_grads, gate_slots, glu_wgrad, lin_wgrad, down_wgrad = lax.map(
        one_expert, (slot_token, slot_pair, w_glu, w_lin, w_down))
    pair_grads = slot_grads.reshape(-1, D)[slot_index].astype(jnp.float32)
    d_tokens = jnp.sum(pair_grads.reshape(TOKENS, TOP, D), axis=1).astype(jnp.bfloat16)
    d_gates = gate_slots.reshape(-1)[slot_index].reshape(TOKENS, TOP)
    glu_norms = jnp.sum(glu_wgrad * glu_wgrad, axis=2)
    lin_norms = jnp.sum(lin_wgrad * lin_wgrad, axis=2)
    down_norms = jnp.sum(down_wgrad * down_wgrad, axis=2)
    return (d_tokens, d_gates, glu_wgrad, lin_wgrad, down_wgrad, glu_norms, lin_norms, down_norms)
```

```python
import functools

import jax
import jax.numpy as jnp
from jax import lax
from jax.experimental import pallas as pl
from jax.experimental.pallas import tpu as pltpu
from jax.sharding import PartitionSpec as P

clamp_limit = 7.0
sigmoid_scale = 1.702
MESH = pl.DeviceIdType.MESH
LANES = 128
CORES = 2
SLABS = 2
f32 = jnp.float32
bf16 = jnp.bfloat16


def dot_nn(a, b):
    return lax.dot_general(a, b, (((1,), (0,)), ((), ())), preferred_element_type=f32)


def dot_nt(a, b):
    return lax.dot_general(a, b, (((1,), (1,)), ((), ())), preferred_element_type=f32)


def flip(index, mask):
    bit = 1
    while bit <= mask:
        if mask & bit:
            index = index + bit - 2 * bit * lax.rem(lax.div(index, bit), 2)
        bit = 2 * bit
    return index


def clamp_backward(glu_pre, lin_pre, back_proj, gate_col):
    glu_clip = jnp.minimum(glu_pre, clamp_limit)
    lin_clip = jnp.clip(lin_pre, -clamp_limit, clamp_limit)
    sig_val = jax.nn.sigmoid(sigmoid_scale * glu_clip)
    glu_act = glu_clip * sig_val
    hidden = glu_act * (lin_clip + 1.0)
    hid_grad = gate_col * back_proj
    act_slope = sig_val + sigmoid_scale * glu_clip * sig_val * (1.0 - sig_val)
    glu_grad = jnp.where(glu_pre < clamp_limit, hid_grad * (lin_clip + 1.0) * act_slope, 0.0)
    lin_grad = jnp.where(jnp.abs(lin_pre) < clamp_limit, hid_grad * glu_act, 0.0)
    return hidden, glu_grad.astype(bf16), lin_grad.astype(bf16)


def piece_list(half):
    narrow = half // 8
    return (
        (1, 0, half // 2, True),
        (0, 0, narrow, True),
        (0, 2 * narrow, half - 2 * narrow, False),
    )


def semaphores(ep, nz, pieces):
    keys = [("load", i) for i in range(7)]
    keys += [(k, 0) for k in ("gs", "ps", "xs", "zs", "as", "bs", "ns")]
    keys += [(k, 0) for k in ("gr", "zr", "ar", "br", "nr")]
    keys += [("ys", a) for a in range(2)]
    for i, piece in enumerate(pieces):
        keys.append(("ds", i))
        if piece[3]:
            keys.append(("hs", i))
        for s in range(SLABS):
            if piece[3]:
                keys += [("dr", i, s, r) for r in range(1, ep)]
                keys.append(("hr", i, s))
            else:
                keys.append(("dr", i, s))
    for s in range(SLABS):
        keys += [("yr", a, s) for a in range(2)]
    for q in range(nz):
        keys.append(("xr", q))
        keys += [("pr", q, s) for s in range(1 + SLABS)]
    return {key: i for i, key in enumerate(keys)}


def kernel(
    ep, tp, cap,
    tok_hbm, routes_hbm, gates_hbm, cot_hbm, wg_hbm, wl_hbm, wd_hbm,
    dtok_ref, dgate_ref, gw_v, lw_v, dw_v, gn_ref, ln_ref, dn_ref,
    tok_ref, routes_ref, gates_ref, cot_ref, wg_ref, wl_ref, wcat_ref, wd_ref,
    pt_v, pk_v, snd_v, all_v, gsnd_v, grow_v, bf_v, hg_v, tr_v,
    ps_v, pr_v, mine_v, xs_v, ret_v, zs_v, zr_v,
    gp_v, gsum_v, gback_v, ns_v, nr_v, sem_v,
):
    me = lax.axis_index("ep")
    tpi = lax.axis_index("tp")
    nz = tp // CORES
    core = lax.rem(tpi, CORES)
    chip = lax.div(tpi, CORES)
    other = 1 - core
    partner = chip * CORES + other
    rows = tok_ref.shape[0]
    width = tok_ref.shape[1]
    units = wd_ref.shape[0]
    half = width // CORES
    own = width // tp
    odd = lax.rem(chip, 2)
    beside = flip(chip, 1) * CORES + core
    span = cap // SLABS
    slab = (ep - 1) * span
    far = SLABS * slab
    pieces = piece_list(half)
    table = semaphores(ep, nz, pieces)

    def sem(*key):
        return sem_v.at[table[key]]

    aligned = units % LANES == 0
    loads = []
    for i, (src, dst) in enumerate((
        (routes_hbm, routes_ref), (gates_hbm, gates_ref), (cot_hbm, cot_ref), (tok_hbm, tok_ref),
        (wg_hbm, wcat_ref.at[:, pl.ds(0, units)] if aligned else wg_ref),
        (wl_hbm, wcat_ref.at[:, pl.ds(units, units)] if aligned else wl_ref),
        (wd_hbm, wd_ref),
    )):
        cp = pltpu.make_async_copy(src, dst, sem("load", i))
        cp.start()
        loads.append(cp)

    barrier = pltpu.get_barrier_semaphore()
    for r in range(1, ep):
        pl.semaphore_signal(barrier, inc=1, device_id={"ep": flip(me, r)}, device_id_type=MESH)
    for q in range(1, tp):
        pl.semaphore_signal(
            barrier, inc=1, device_id={"tp": lax.rem(tpi + q, tp)}, device_id_type=MESH
        )

    def remote(src, dst, ss, rs, where):
        return pltpu.make_async_remote_copy(
            src_ref=src, dst_ref=dst, send_sem=ss, recv_sem=rs,
            device_id=where, device_id_type=MESH,
        )

    def arrived(ref, *key):
        remote(ref, ref, sem(*key), sem(*key), {"tp": partner}).wait_recv()

    def sent(ref, *key):
        remote(ref, ref, sem(*key), sem(*key), {"tp": partner}).wait_send()

    loads[0].wait()
    loads[1].wait()
    rel = jnp.bitwise_xor(routes_ref[...], me)
    erows = gp_v.shape[1]
    sub = lax.broadcasted_iota(jnp.int32, (erows, rows), 0)
    first, second = sub == rel[0:1, :], sub == rel[1:2, :]
    mask = jnp.where(first, 1.0, 0.0) + jnp.where(second, 1.0, 0.0)
    gate_of = jnp.where(first, gates_ref[0:1, :], 0.0) + jnp.where(second, gates_ref[1:2, :], 0.0)
    before = lax.broadcasted_iota(jnp.int32, (rows, rows), 0) < lax.broadcasted_iota(
        jnp.int32, (rows, rows), 1
    )
    rank = dot_nn(mask.astype(bf16), jnp.where(before, 1.0, 0.0).astype(bf16))
    place = jnp.where(mask > 0.5, rank, -1.0)
    slot_at = lax.broadcasted_iota(jnp.int32, (LANES, rows), 0).astype(f32)
    hits = [jnp.where(slot_at == place[r:r + 1, :], 1.0, 0.0) for r in range(ep)]
    outgoing = [
        jnp.concatenate([hits[r][s * span:(s + 1) * span, :] for r in range(1, ep)], axis=0)
        for s in range(SLABS)
    ]
    picks = [x.astype(bf16) for x in outgoing]
    square = lax.broadcasted_iota(jnp.int32, (LANES, LANES), 0) == lax.broadcasted_iota(
        jnp.int32, (LANES, LANES), 1
    )
    swapped = [i for i, piece in enumerate(pieces) if piece[3]]
    refs = (tok_ref, cot_ref)

    def window(i, whose):
        a, off, w, shared = pieces[i]
        if shared:
            off = off + whose * w
        return a, (pl.ds(pl.multiple_of(off, LANES), w) if shared else pl.ds(off, w))

    def block(s, r):
        return pl.ds(cap + s * slab + (r - 1) * span, span)

    def area(i, at, whose):
        a, cols = window(i, whose)
        return all_v.at[a, core, at, cols]

    def relay(i, s, whose):
        a = pieces[i][0]
        at = area(i, pl.ds(cap + s * slab, slab), whose)
        remote(at, at, sem("ys", a), sem("yr", a, s), {"tp": partner}).start()

    loads[2].wait()
    loads[3].wait()
    waited = False
    for s in range(SLABS):
        for i in range(len(pieces)):
            a, off, w, shared = pieces[i]
            cols = window(i, odd)[1]
            begin = core * half + off + (odd * w if shared else 0)
            src_cols = pl.ds(pl.multiple_of(begin, LANES), w)
            snd_v[a, s * slab:(s + 1) * slab, cols] = dot_nn(
                picks[s], refs[a][:, src_cols]
            ).astype(bf16)
            if not waited:
                pl.semaphore_wait(barrier, ep - 1 + tp - 1)
                waited = True
            for r in reversed(range(1, ep)):
                key = ("dr", i, s, r) if shared else ("dr", i, s)
                remote(
                    snd_v.at[a, pl.ds(s * slab + (r - 1) * span, span), cols],
                    area(i, block(s, r), odd), sem("ds", i), sem(*key), {"ep": flip(me, r)},
                ).start()
    for r in range(ep):
        col = jnp.sum(hits[r] * gate_of[r:r + 1, :], axis=1, keepdims=True)
        row = jnp.sum(jnp.where(square, col, 0.0), axis=0, keepdims=True)
        if r == 0:
            grow_v[0] = jnp.broadcast_to(row, (8, LANES))
        else:
            gsnd_v[r] = jnp.broadcast_to(row, (8, LANES))
            remote(
                gsnd_v.at[r], grow_v.at[r], sem("gs", 0), sem("gr", 0), {"ep": flip(me, r)}
            ).start()
    home = hits[0][:cap, :].astype(bf16)
    for a, ref in ((0, tok_ref), (1, cot_ref)):
        for h in range(CORES):
            all_v[a, h, 0:cap, :] = dot_nn(home, ref[:, h * half:(h + 1) * half]).astype(bf16)
    for r in range(ep):
        pk_v[r] = hits[r].astype(bf16)
    pt_v[...] = jnp.concatenate([hits[0][:cap, :]] + outgoing, axis=0).T.astype(bf16)

    gp_v[tpi] = jnp.zeros(gp_v.shape[1:], f32)

    def forward(at, count, blocks, shift, ready):
        eye = lax.broadcasted_iota(jnp.int32, (count, LANES), 0) + shift == (
            lax.broadcasted_iota(jnp.int32, (count, LANES), 1)
        )
        rs = slice(at, at + count * len(blocks))
        n = rs.stop - rs.start
        ready(1)
        back = jnp.zeros((n, units), f32)
        for h in range(CORES):
            back = back + dot_nt(all_v[1, h, rs, :], wd_ref[:, h * half:(h + 1) * half])
        gate_col = jnp.concatenate([
            jnp.sum(jnp.where(eye, grow_v[r, 0:1, :], 0.0), axis=1, keepdims=True)
            for r in blocks
        ], axis=0)
        ready(0)
        pre = jnp.zeros((n, 2 * units), f32)
        for h in range(CORES):
            pre = pre + dot_nn(all_v[0, h, rs, :], wcat_ref[h * half:(h + 1) * half, :])
        hidden, glu_bf, lin_bf = clamp_backward(
            pre[:, 0:units], pre[:, units:2 * units], back, gate_col
        )
        part = jnp.sum(back * hidden, axis=1, keepdims=True)
        bf_v[rs, 0:units] = glu_bf
        bf_v[rs, units:2 * units] = lin_bf
        hg_v[rs, :] = (gate_col * hidden).astype(bf16)
        for k, r in enumerate(blocks):
            line = jnp.sum(
                jnp.where(eye, part[k * count:(k + 1) * count, :], 0.0), axis=0, keepdims=True
            )
            gp_v[tpi, r:r + 1, :] = gp_v[tpi, r:r + 1, :] + line

    order = list(reversed(range(1, nz))) + [0]

    def input_cols(k, which, rs):
        at = pl.ds(pl.multiple_of((flip(chip, k) * CORES + which) * own, own), own)
        return dot_nt(bf_v[rs, :], wcat_ref[at, :])

    def give(b, rs):
        at = pl.ds(rs.start, rs.stop - rs.start)
        for q in order:
            ps_v[q, rs, :] = input_cols(q, other, rs).astype(bf16)
            remote(
                ps_v.at[q, at, :], pr_v.at[q, at, :], sem("ps", 0), sem("pr", q, b),
                {"tp": partner},
            ).start()
        for q in order:
            mine_v[q, rs, :] = input_cols(q, core, rs)

    def take(b, rs):
        at = pl.ds(rs.start, rs.stop - rs.start)
        for q in order:
            arrived(pr_v.at[q, at, :], "pr", q, b)
            total = (mine_v[q, rs, :] + pr_v[q, rs, :].astype(f32)).astype(bf16)
            if b == 0:
                ret_v[q, rs, :] = total
                continue
            xs_v[q, rs, :] = total
            for r in reversed(range(1, ep)):
                where = block(b - 1, r)
                remote(
                    xs_v.at[q, where, :], ret_v.at[q, where, :],
                    sem("xs", 0), sem("xr", q), {"ep": flip(me, r)},
                ).start()

    def slab_rows(s):
        return slice(cap + s * slab, cap + (s + 1) * slab)

    def pass_shared(s):
        for i in swapped:
            for r in reversed(range(1, ep)):
                at = area(i, block(s, r), odd)
                arrived(at, "dr", i, s, r)
                remote(at, at, sem("hs", i), sem("hr", i, s), {"tp": beside}).start()
            relay(i, s, odd)

    def pass_rest(s):
        whole = pl.ds(cap + s * slab, slab)
        for i in range(len(pieces)):
            if i in swapped:
                arrived(area(i, whole, 1 - odd), "hr", i, s)
                relay(i, s, 1 - odd)
        for i in range(len(pieces)):
            if i not in swapped:
                arrived(area(i, whole, odd), "dr", i, s)
                relay(i, s, odd)

    def landed(s):
        def ready(a):
            arrived(all_v.at[a, other, pl.ds(cap + s * slab, slab), :], "yr", a, s)
        return ready

    home_rows = slice(0, cap)
    remote_blocks = list(range(1, ep))
    pass_shared(0)
    for cp in loads[4:]:
        cp.wait()
    if not aligned:
        wcat_ref[...] = jnp.concatenate([wg_ref[...], wl_ref[...]], axis=1)
    forward(0, cap, [0], 0, lambda a: None)
    give(0, home_rows)
    pass_rest(0)
    arrived(grow_v.at[pl.ds(1, ep - 1)], "gr", 0)
    for s in range(SLABS):
        forward(cap + s * slab, span, remote_blocks, s * span, landed(s))
        give(1 + s, slab_rows(s))
        if s == 0:
            take(0, home_rows)
        if s + 1 < SLABS:
            pass_shared(s + 1)
        take(1 + s, slab_rows(s))
        if s + 1 < SLABS:
            pass_rest(s + 1)

    for q in range(1, tp):
        remote(
            gp_v.at[tpi], gp_v.at[tpi], sem("as", 0), sem("ar", 0),
            {"tp": lax.rem(tpi + q, tp)},
        ).start()

    tr_v[0:2 * units, :] = bf_v[...].astype(f32).T.astype(bf16)
    tr_v[2 * units:3 * units, :] = hg_v[...].astype(f32).T.astype(bf16)
    step = min(512, half)
    for h in range(CORES):
        for c0 in range(0, half, step):
            cols = slice(h * half + c0, h * half + c0 + step)
            w = dot_nn(tr_v[0:2 * units, :], all_v[0, h, :, c0:c0 + step])
            for n, w_v in enumerate((gw_v, lw_v)):
                wn = w[n * units:(n + 1) * units, :]
                ns_v[n:n + 1, cols] = jnp.sum(wn * wn, axis=0, keepdims=True)
                w_v[cols, :] = wn.T
    nr_v[tpi] = ns_v[...]
    for q in range(1, tp):
        remote(
            ns_v, nr_v.at[tpi], sem("ns", 0), sem("nr", 0), {"tp": lax.rem(tpi + q, tp)}
        ).start()

    arrived(gp_v.at[pl.ds(1, tp - 1)], "ar", 0)
    gsum = gp_v[0]
    for j in range(1, tp):
        gsum = gsum + gp_v[j]
    gback_v[0, 0:1, :] = gsum[0:1, :]
    for r in range(1, ep):
        gsum_v[r] = jnp.broadcast_to(gsum[r:r + 1, :], (8, LANES))
        remote(
            gsum_v.at[r], gback_v.at[r], sem("bs", 0), sem("br", 0), {"ep": flip(me, r)}
        ).start()

    norm = jnp.zeros((units, 1), f32)
    for h in range(CORES):
        for c0 in range(0, half, step):
            cols = slice(h * half + c0, h * half + c0 + step)
            w = dot_nn(tr_v[2 * units:3 * units, :], all_v[1, h, :, c0:c0 + step])
            norm = norm + jnp.sum(w * w, axis=1, keepdims=True)
            dw_v[:, cols] = w
    diag = lax.broadcasted_iota(jnp.int32, (units, units), 0) == (
        lax.broadcasted_iota(jnp.int32, (units, units), 1)
    )
    dn_ref[...] = jnp.sum(jnp.where(diag, norm, 0.0), axis=0, keepdims=True)

    acc = None
    for q in order:
        arrived(ret_v.at[q, pl.ds(cap, far), :], "xr", q)
        part = dot_nn(pt_v[...], ret_v[q])
        if q == 0:
            acc = part
        else:
            zs_v[q] = part.astype(bf16)
            remote(
                zs_v.at[q], zr_v.at[q], sem("zs", 0), sem("zr", 0),
                {"tp": flip(chip, q) * CORES + core},
            ).start()

    arrived(gback_v.at[pl.ds(1, ep - 1)], "br", 0)
    res = [jnp.zeros((1, rows), f32), jnp.zeros((1, rows), f32)]
    for r in range(ep):
        col = jnp.sum(jnp.where(square, gback_v[r, 0:1, :], 0.0), axis=1, keepdims=True)
        val = jnp.sum(pk_v[r].astype(f32) * col, axis=0, keepdims=True)
        for k in range(2):
            res[k] = res[k] + jnp.where(rel[k:k + 1, :] == r, val, 0.0)
    dgate_ref[0:1, :] = res[0]
    dgate_ref[1:2, :] = res[1]

    arrived(nr_v.at[pl.ds(1, tp - 1)], "nr", 0)
    norms = nr_v[0]
    for j in range(1, tp):
        norms = norms + nr_v[j]
    gn_ref[...] = norms[0:1, :]
    ln_ref[...] = norms[1:2, :]

    if nz > 1:
        arrived(zr_v.at[pl.ds(1, nz - 1)], "zr", 0)
    for q in range(1, nz):
        acc = acc + zr_v[q].astype(f32)
    dtok_ref[...] = acc.astype(bf16)

    remote_rows = pl.ds(cap, far)
    for i in range(len(pieces)):
        a, cols = window(i, odd)
        sent(snd_v.at[a, :, cols], "ds", i)
        if i in swapped:
            sent(area(i, remote_rows, odd), "hs", i)
    for a in range(2):
        sent(all_v.at[a, core, remote_rows, :], "ys", a)
    sent(gsnd_v.at[pl.ds(1, ep - 1)], "gs", 0)
    sent(ps_v, "ps", 0)
    sent(xs_v.at[:, remote_rows, :], "xs", 0)
    if nz > 1:
        sent(zs_v.at[pl.ds(1, nz - 1)], "zs", 0)
    sent(gp_v.at[pl.ds(1, tp - 1)], "as", 0)
    sent(gsum_v.at[pl.ds(1, ep - 1)], "bs", 0)
    sent(nr_v.at[pl.ds(1, tp - 1)], "ns", 0)


def write_out(*refs):
    count = (len(refs) - 1) // 2
    copies = [
        pltpu.make_async_copy(refs[i], refs[count + i], refs[-1].at[i]) for i in range(count)
    ]
    for cp in copies:
        cp.start()
    for cp in copies:
        cp.wait()


def shards(tokens, routes, gates, cotangent, w_glu, w_lin, w_down):
    ep = lax.axis_size("ep")
    tp = lax.axis_size("tp")
    rows, top = routes.shape
    width = tokens.shape[1]
    units = w_glu.shape[2]
    cap = 3 * rows * top // (2 * ep)
    cap = -(-cap // (16 * SLABS)) * (16 * SLABS)
    slots = ep * cap
    half = width // CORES
    own = width // tp
    nz = tp // CORES
    vm = pl.BlockSpec(memory_space=pltpu.VMEM)
    hbm = pl.BlockSpec(memory_space=pltpu.HBM)
    dma = pltpu.SemaphoreType.DMA
    erows = max(8, ep)
    V = pltpu.VMEM
    out_shape = (
        jax.ShapeDtypeStruct((rows, own), bf16),
        jax.ShapeDtypeStruct((top, rows), f32),
        jax.ShapeDtypeStruct((width, units), f32),
        jax.ShapeDtypeStruct((width, units), f32),
        jax.ShapeDtypeStruct((units, width), f32),
        jax.ShapeDtypeStruct((1, width), f32),
        jax.ShapeDtypeStruct((1, width), f32),
        jax.ShapeDtypeStruct((1, units), f32),
    )
    outs = pl.pallas_call(
        functools.partial(kernel, ep, tp, cap),
        out_shape=out_shape,
        in_specs=[hbm] * 7,
        out_specs=(vm,) * 8,
        scratch_shapes=[
            V((rows, width), bf16),
            V((top, rows), jnp.int32),
            V((top, rows), f32),
            V((rows, width), bf16),
            V((width, units) if units % LANES else (16, LANES), bf16),
            V((width, units) if units % LANES else (16, LANES), bf16),
            V((width, 2 * units), bf16),
            V((units, width), bf16),
            V((rows, slots), bf16),
            V((ep, LANES, rows), bf16),
            V((2, slots - cap, half), bf16),
            V((2, CORES, slots, half), bf16),
            V((ep, 8, LANES), f32),
            V((ep, 8, LANES), f32),
            V((slots, 2 * units), bf16),
            V((slots, units), bf16),
            V((3 * units, slots), bf16),
            V((nz, slots, own), bf16),
            V((nz, slots, own), bf16),
            V((nz, slots, own), f32),
            V((nz, slots, own), bf16),
            V((nz, slots, own), bf16),
            V((nz, rows, own), bf16),
            V((nz, rows, own), bf16),
            V((tp, erows, LANES), f32),
            V((ep, 8, LANES), f32),
            V((ep, 8, LANES), f32),
            V((2, width), f32),
            V((tp, 2, width), f32),
            dma((len(semaphores(ep, nz, piece_list(half))),)),
        ],
        compiler_params=pltpu.CompilerParams(
            collective_id=0, has_side_effects=True, vmem_limit_bytes=28 * 1024 * 1024
        ),
    )(*(pltpu.with_memory_space_constraint(x, pltpu.HBM) for x in (
        tokens, routes.T, gates.T, cotangent, w_glu[0], w_lin[0], w_down[0]
    )))
    outs = pl.pallas_call(
        write_out,
        out_shape=out_shape,
        in_specs=[vm] * len(out_shape),
        out_specs=(hbm,) * len(out_shape),
        scratch_shapes=[dma((len(out_shape),))],
        compiler_params=pltpu.CompilerParams(vmem_limit_bytes=28 * 1024 * 1024),
    )(*outs)
    d_tokens, d_gates, gw, lw, dw, gn, ln, dn = outs
    return (d_tokens, d_gates.T, gw[None], lw[None], dw[None], gn, ln, dn)


def solution(mesh):
    in_specs = (
        P("ep", None),
        P("ep", None),
        P("ep", None),
        P("ep", None),
        P("ep", None, "tp"),
        P("ep", None, "tp"),
        P("ep", "tp", None),
    )
    out_specs = (
        P("ep", "tp"),
        P("ep", None),
        P("ep", None, "tp"),
        P("ep", None, "tp"),
        P("ep", "tp", None),
        P("ep", None),
        P("ep", None),
        P("ep", "tp"),
    )
    return jax.shard_map(shards, mesh=mesh, in_specs=in_specs, out_specs=out_specs, check_vma=False)
```

```python
import functools

import jax
import jax.numpy as jnp
from jax import lax
from jax.experimental import pallas as pl
from jax.experimental.pallas import tpu as pltpu
from jax.sharding import PartitionSpec as P

clamp_limit = 7.0
sigmoid_scale = 1.702
MESH = pl.DeviceIdType.MESH
LANES = 128
CORES = 2
SHARE = 3
FLIGHT = 6
f32 = jnp.float32
bf16 = jnp.bfloat16


def dot_nn(a, b):
    return lax.dot_general(a, b, (((1,), (0,)), ((), ())), preferred_element_type=f32)


def dot_nt(a, b):
    return lax.dot_general(a, b, (((1,), (1,)), ((), ())), preferred_element_type=f32)


def flip(index, mask):
    bit = 1
    while bit <= mask:
        if mask & bit:
            index = index + bit - 2 * bit * lax.rem(lax.div(index, bit), 2)
        bit = 2 * bit
    return index


def clamp_backward(glu_pre, lin_pre, back_proj, gate_col):
    glu_clip = jnp.minimum(glu_pre, clamp_limit)
    lin_clip = jnp.clip(lin_pre, -clamp_limit, clamp_limit)
    sig_val = jax.nn.sigmoid(sigmoid_scale * glu_clip)
    glu_act = glu_clip * sig_val
    hidden = glu_act * (lin_clip + 1.0)
    hid_grad = gate_col * back_proj
    act_slope = sig_val + sigmoid_scale * glu_clip * sig_val * (1.0 - sig_val)
    glu_grad = jnp.where(glu_pre < clamp_limit, hid_grad * (lin_clip + 1.0) * act_slope, 0.0)
    lin_grad = jnp.where(jnp.abs(lin_pre) < clamp_limit, hid_grad * glu_act, 0.0)
    return hidden, glu_grad.astype(bf16), lin_grad.astype(bf16)


def slab_cuts(cap):
    first = min(-(-2 * cap // 48) * 16, cap - 16)
    return (first, cap - first)


def piece_list(half):
    unit = half // 8
    early = tuple((1, 2 * k * unit, unit, True) for k in range(4)) + (
        (0, 0, unit, True),
    ) + tuple((0, (2 + 2 * k) * unit, 2 * unit, False) for k in range(3))
    late = (
        (1, 0, SHARE * unit, True),
        (1, 2 * SHARE * unit, half - 2 * SHARE * unit, False),
        (0, 0, half // 2, False),
        (0, half // 2, half // 2, False),
    )
    return (early, late)


def semaphores(ep, nz, plan):
    keys = [("load", i) for i in range(7)]
    keys += [(k, 0) for k in ("gs", "ps", "xs", "zs", "as", "bs", "ns", "ds", "hs", "ys")]
    keys += [(k, 0) for k in ("gr", "ar", "br", "nr")]
    for s, pieces in enumerate(plan):
        for i, piece in enumerate(pieces):
            keys.append(("dr", s, i))
            if piece[3]:
                keys.append(("hr", s, i))
        keys += [("yr", s, a) for a in range(2)]
        keys.append(("zr", s))
    for q in range(nz):
        keys += [("pr", q, b) for b in range(1 + len(plan))]
        keys += [("xr", q, s) for s in range(len(plan))]
    return {key: i for i, key in enumerate(keys)}


def kernel(
    ep, tp, cap,
    tok_hbm, routes_hbm, gates_hbm, cot_hbm, wg_hbm, wl_hbm, wd_hbm,
    dtok_ref, dgate_ref, gw_v, lw_v, dw_v, gn_ref, ln_ref, dn_ref,
    tok_ref, routes_ref, gates_ref, cot_ref, wg_ref, wl_ref, wcat_ref, wd_ref,
    pt_v, pk_v, snd_v, all_v, gsnd_v, grow_v, bf_v, hg_v, tr_v,
    ps_v, pr_v, xs_v, ret_v, zs_v, zr_v,
    gp_v, gsum_v, gback_v, ns_v, nr_v, sem_v,
):
    me = lax.axis_index("ep")
    tpi = lax.axis_index("tp")
    nz = tp // CORES
    core = lax.rem(tpi, CORES)
    chip = lax.div(tpi, CORES)
    other = 1 - core
    partner = chip * CORES + other
    rows = tok_ref.shape[0]
    width = tok_ref.shape[1]
    units = wd_ref.shape[0]
    half = width // CORES
    own = width // tp
    odd = lax.rem(chip, 2)
    beside = flip(chip, 1) * CORES + core
    cuts = slab_cuts(cap)
    slabs = [(ep - 1) * n for n in cuts]
    bases = [cap + sum(slabs[:s]) for s in range(len(cuts))]
    ranks = [sum(cuts[:s]) for s in range(len(cuts))]
    far = sum(slabs)
    plan = piece_list(half)
    table = semaphores(ep, nz, plan)

    def sem(*key):
        return sem_v.at[table[key]]

    aligned = units % LANES == 0
    loads = []
    for i, (src, dst) in enumerate((
        (routes_hbm, routes_ref), (gates_hbm, gates_ref), (cot_hbm, cot_ref), (tok_hbm, tok_ref),
        (wg_hbm, wcat_ref.at[:, pl.ds(0, units)] if aligned else wg_ref),
        (wl_hbm, wcat_ref.at[:, pl.ds(units, units)] if aligned else wl_ref),
        (wd_hbm, wd_ref),
    )):
        cp = pltpu.make_async_copy(src, dst, sem("load", i))
        cp.start()
        loads.append(cp)

    barrier = pltpu.get_barrier_semaphore()
    for r in range(1, ep):
        pl.semaphore_signal(barrier, inc=1, device_id={"ep": flip(me, r)}, device_id_type=MESH)
    for q in range(1, tp):
        pl.semaphore_signal(
            barrier, inc=1, device_id={"tp": lax.rem(tpi + q, tp)}, device_id_type=MESH
        )

    def remote(src, dst, ss, rs, where):
        return pltpu.make_async_remote_copy(
            src_ref=src, dst_ref=dst, send_sem=ss, recv_sem=rs,
            device_id=where, device_id_type=MESH,
        )

    def arrived(ref, *key):
        remote(ref, ref, sem(*key), sem(*key), {"tp": partner}).wait_recv()

    def sent(ref, *key):
        remote(ref, ref, sem(*key), sem(*key), {"tp": partner}).wait_send()

    loads[0].wait()
    loads[1].wait()
    rel = jnp.bitwise_xor(routes_ref[...], me)
    erows = gp_v.shape[1]
    sub = lax.broadcasted_iota(jnp.int32, (erows, rows), 0)
    first, second = sub == rel[0:1, :], sub == rel[1:2, :]
    mask = jnp.where(first, 1.0, 0.0) + jnp.where(second, 1.0, 0.0)
    gate_of = jnp.where(first, gates_ref[0:1, :], 0.0) + jnp.where(second, gates_ref[1:2, :], 0.0)
    before = lax.broadcasted_iota(jnp.int32, (rows, rows), 0) < lax.broadcasted_iota(
        jnp.int32, (rows, rows), 1
    )
    rank = dot_nn(mask.astype(bf16), jnp.where(before, 1.0, 0.0).astype(bf16))
    place = jnp.where(mask > 0.5, rank, -1.0)
    slot_at = lax.broadcasted_iota(jnp.int32, (LANES, rows), 0).astype(f32)
    hits = [jnp.where(slot_at == place[r:r + 1, :], 1.0, 0.0) for r in range(ep)]
    outgoing = [
        jnp.concatenate([hits[r][at:at + n, :] for r in range(1, ep)], axis=0)
        for at, n in zip(ranks, cuts)
    ]
    picks = [x.astype(bf16) for x in outgoing]
    square = lax.broadcasted_iota(jnp.int32, (LANES, LANES), 0) == lax.broadcasted_iota(
        jnp.int32, (LANES, LANES), 1
    )
    refs = (tok_ref, cot_ref)

    def window(s, i, whose):
        a, off, w, shared = plan[s][i]
        if shared:
            return a, pl.ds(pl.multiple_of(off + whose * w, LANES), w)
        return a, pl.ds(off, w)

    def block(s, r):
        return pl.ds(bases[s] + (r - 1) * cuts[s], cuts[s])

    def whole(s):
        return pl.ds(bases[s], slabs[s])

    def area(s, i, at, whose):
        a, cols = window(s, i, whose)
        return all_v.at[a, core, at, cols]

    def relay(s, i, whose):
        at = area(s, i, whole(s), whose)
        remote(at, at, sem("ys", 0), sem("yr", s, plan[s][i][0]), {"tp": partner}).start()

    steps = [(s, i) for s in range(len(cuts)) for i in range(len(plan[s]))]
    state = {"next": 0, "load": 0, "waited": False}

    def cost(s, i):
        return cuts[s] * plan[s][i][2]

    def dispatch():
        s, i = steps[state["next"]]
        a, off, w, shared = plan[s][i]
        cols = window(s, i, odd)[1]
        begin = core * half + off + (odd * w if shared else 0)
        src_cols = pl.ds(pl.multiple_of(begin, LANES), w)
        at = bases[s] - cap
        snd_v[a, at:at + slabs[s], cols] = dot_nn(picks[s], refs[a][:, src_cols]).astype(bf16)
        if not state["waited"]:
            pl.semaphore_wait(barrier, ep - 1 + tp - 1)
            state["waited"] = True
        for r in reversed(range(1, ep)):
            remote(
                snd_v.at[a, pl.ds(at + (r - 1) * cuts[s], cuts[s]), cols],
                area(s, i, block(s, r), odd), sem("ds", 0), sem("dr", s, i), {"ep": flip(me, r)},
            ).start()
        state["next"] += 1
        state["load"] += cost(s, i)

    def fill():
        while state["next"] < len(steps) and state["load"] < FLIGHT * cuts[0] * half // 8:
            dispatch()

    def land(s, i):
        at = area(s, i, whole(s), odd)
        arrived(at, "dr", s, i)
        if plan[s][i][3]:
            remote(at, at, sem("hs", 0), sem("hr", s, i), {"tp": beside}).start()
        relay(s, i, odd)
        state["load"] -= cost(s, i)
        fill()

    def turn(s, i):
        arrived(area(s, i, whole(s), 1 - odd), "hr", s, i)
        relay(s, i, 1 - odd)

    loads[2].wait()
    loads[3].wait()
    fill()
    for r in range(ep):
        col = jnp.sum(hits[r] * gate_of[r:r + 1, :], axis=1, keepdims=True)
        row = jnp.sum(jnp.where(square, col, 0.0), axis=0, keepdims=True)
        if r == 0:
            grow_v[0] = jnp.broadcast_to(row, (8, LANES))
        else:
            gsnd_v[r] = jnp.broadcast_to(row, (8, LANES))
            remote(
                gsnd_v.at[r], grow_v.at[r], sem("gs", 0), sem("gr", 0), {"ep": flip(me, r)}
            ).start()
    home = hits[0][:cap, :].astype(bf16)
    for a, ref in ((0, tok_ref), (1, cot_ref)):
        for h in range(CORES):
            all_v[a, h, 0:cap, :] = dot_nn(home, ref[:, h * half:(h + 1) * half]).astype(bf16)
    for r in range(ep):
        pk_v[r] = hits[r].astype(bf16)
    pt_v[...] = jnp.concatenate([hits[0][:cap, :]] + outgoing, axis=0).T.astype(bf16)

    gp_v[tpi] = jnp.zeros(gp_v.shape[1:], f32)

    def forward(at, count, blocks, shift, ready):
        eye = lax.broadcasted_iota(jnp.int32, (count, LANES), 0) + shift == (
            lax.broadcasted_iota(jnp.int32, (count, LANES), 1)
        )
        rs = slice(at, at + count * len(blocks))
        n = rs.stop - rs.start
        ready(1)
        back = jnp.zeros((n, units), f32)
        for h in range(CORES):
            back = back + dot_nt(all_v[1, h, rs, :], wd_ref[:, h * half:(h + 1) * half])
        gate_col = jnp.concatenate([
            jnp.sum(jnp.where(eye, grow_v[r, 0:1, :], 0.0), axis=1, keepdims=True)
            for r in blocks
        ], axis=0)
        ready(0)
        pre = jnp.zeros((n, 2 * units), f32)
        for h in range(CORES):
            pre = pre + dot_nn(all_v[0, h, rs, :], wcat_ref[h * half:(h + 1) * half, :])
        hidden, glu_bf, lin_bf = clamp_backward(
            pre[:, 0:units], pre[:, units:2 * units], back, gate_col
        )
        part = jnp.sum(back * hidden, axis=1, keepdims=True)
        bf_v[rs, 0:units] = glu_bf
        bf_v[rs, units:2 * units] = lin_bf
        hg_v[rs, :] = (gate_col * hidden).astype(bf16)
        for k, r in enumerate(blocks):
            line = jnp.sum(
                jnp.where(eye, part[k * count:(k + 1) * count, :], 0.0), axis=0, keepdims=True
            )
            gp_v[tpi, r:r + 1, :] = gp_v[tpi, r:r + 1, :] + line

    order = list(reversed(range(1, nz))) + [0]

    def input_cols(k, which, rs):
        at = pl.ds(pl.multiple_of((flip(chip, k) * CORES + which) * own, own), own)
        return dot_nt(bf_v[rs, :], wcat_ref[at, :])

    def give(b, rs):
        at = pl.ds(rs.start, rs.stop - rs.start)
        for q in order:
            ps_v[q, rs, :] = input_cols(q, other, rs).astype(bf16)
            remote(
                ps_v.at[q, at, :], pr_v.at[q, at, :], sem("ps", 0), sem("pr", q, b),
                {"tp": partner},
            ).start()

    def take(b, rs):
        at = pl.ds(rs.start, rs.stop - rs.start)
        for q in order:
            mine = input_cols(q, core, rs)
            arrived(pr_v.at[q, at, :], "pr", q, b)
            total = (mine + pr_v[q, rs, :].astype(f32)).astype(bf16)
            if b == 0:
                ret_v[q, rs, :] = total
                continue
            xs_v[q, rs, :] = total
            for r in reversed(range(1, ep)):
                where = block(b - 1, r)
                remote(
                    xs_v.at[q, where, :], ret_v.at[q, where, :],
                    sem("xs", 0), sem("xr", q, b - 1), {"ep": flip(me, r)},
                ).start()

    def slab_rows(s):
        return slice(bases[s], bases[s] + slabs[s])

    def landed(s):
        def ready(a):
            arrived(all_v.at[a, other, whole(s), :], "yr", s, a)
        return ready

    def is_shared(s):
        return [i for i, piece in enumerate(plan[s]) if piece[3]]

    home_rows = slice(0, cap)
    remote_blocks = list(range(1, ep))
    for cp in loads[4:]:
        cp.wait()
    if not aligned:
        wcat_ref[...] = jnp.concatenate([wg_ref[...], wl_ref[...]], axis=1)
    forward(0, cap, [0], 0, lambda a: None)
    give(0, home_rows)
    lag = 2
    turns = []
    for i in range(len(plan[0])):
        land(0, i)
        if plan[0][i][3]:
            turns.append(i)
        while len(turns) > lag or (turns and not plan[0][i][3]):
            turn(0, turns.pop(0))
    take(0, home_rows)
    for i in is_shared(1):
        land(1, i)
    arrived(grow_v.at[pl.ds(1, ep - 1)], "gr", 0)
    forward(bases[0], cuts[0], remote_blocks, ranks[0], landed(0))
    give(1, slab_rows(0))
    rest = [i for i in range(len(plan[1])) if not plan[1][i][3]]
    for i in rest[:-1]:
        land(1, i)
    for i in is_shared(1):
        turn(1, i)
    take(1, slab_rows(0))
    land(1, rest[-1])
    forward(bases[1], cuts[1], remote_blocks, ranks[1], landed(1))
    give(2, slab_rows(1))
    take(2, slab_rows(1))

    for q in range(1, tp):
        remote(
            gp_v.at[tpi], gp_v.at[tpi], sem("as", 0), sem("ar", 0),
            {"tp": lax.rem(tpi + q, tp)},
        ).start()

    marks = [0, ranks[1], rows]

    def combine(s):
        kept = None
        lines = slice(marks[s], marks[s + 1])
        at = pl.ds(marks[s], marks[s + 1] - marks[s])
        deep = bases[s] + slabs[s]
        for q in order:
            arrived(ret_v.at[q, whole(s), :], "xr", q, s)
            part = dot_nn(pt_v[lines, 0:deep], ret_v[q, 0:deep, :])
            if q == 0:
                kept = part
                continue
            zs_v[q, lines, :] = part.astype(bf16)
            remote(
                zs_v.at[q, at, :], zr_v.at[q, at, :], sem("zs", 0), sem("zr", s),
                {"tp": flip(chip, q) * CORES + core},
            ).start()
        return kept

    kept = [combine(0)]
    tr_v[0:2 * units, :] = bf_v[...].astype(f32).T.astype(bf16)
    tr_v[2 * units:3 * units, :] = hg_v[...].astype(f32).T.astype(bf16)
    step = min(512, half)
    for h in range(CORES):
        for c0 in range(0, half, step):
            cols = slice(h * half + c0, h * half + c0 + step)
            w = dot_nn(tr_v[0:2 * units, :], all_v[0, h, :, c0:c0 + step])
            for n, w_v in enumerate((gw_v, lw_v)):
                wn = w[n * units:(n + 1) * units, :]
                ns_v[n:n + 1, cols] = jnp.sum(wn * wn, axis=0, keepdims=True)
                w_v[cols, :] = wn.T
    nr_v[tpi] = ns_v[...].astype(bf16)
    for q in range(1, tp):
        remote(
            nr_v.at[tpi], nr_v.at[tpi], sem("ns", 0), sem("nr", 0),
            {"tp": lax.rem(tpi + q, tp)},
        ).start()

    arrived(gp_v.at[pl.ds(1, tp - 1)], "ar", 0)
    gsum = gp_v[0]
    for j in range(1, tp):
        gsum = gsum + gp_v[j]
    gback_v[0, 0:1, :] = gsum[0:1, :]
    for r in range(1, ep):
        gsum_v[r] = jnp.broadcast_to(gsum[r:r + 1, :], (8, LANES))
        remote(
            gsum_v.at[r], gback_v.at[r], sem("bs", 0), sem("br", 0), {"ep": flip(me, r)}
        ).start()
    norm = jnp.zeros((units, 1), f32)
    for h in range(CORES):
        for c0 in range(0, half, step):
            cols = slice(h * half + c0, h * half + c0 + step)
            w = dot_nn(tr_v[2 * units:3 * units, :], all_v[1, h, :, c0:c0 + step])
            norm = norm + jnp.sum(w * w, axis=1, keepdims=True)
            dw_v[:, cols] = w
    diag = lax.broadcasted_iota(jnp.int32, (units, units), 0) == (
        lax.broadcasted_iota(jnp.int32, (units, units), 1)
    )
    dn_ref[...] = jnp.sum(jnp.where(diag, norm, 0.0), axis=0, keepdims=True)

    kept.append(combine(1))
    arrived(gback_v.at[pl.ds(1, ep - 1)], "br", 0)
    res = [jnp.zeros((1, rows), f32), jnp.zeros((1, rows), f32)]
    for r in range(ep):
        col = jnp.sum(jnp.where(square, gback_v[r, 0:1, :], 0.0), axis=1, keepdims=True)
        val = jnp.sum(pk_v[r].astype(f32) * col, axis=0, keepdims=True)
        for k in range(2):
            res[k] = res[k] + jnp.where(rel[k:k + 1, :] == r, val, 0.0)
    dgate_ref[0:1, :] = res[0]
    dgate_ref[1:2, :] = res[1]

    arrived(nr_v.at[pl.ds(1, tp - 1)], "nr", 0)
    norms = nr_v[0].astype(f32)
    for j in range(1, tp):
        norms = norms + nr_v[j].astype(f32)
    gn_ref[...] = norms[0:1, :]
    ln_ref[...] = norms[1:2, :]

    for s in range(len(cuts)):
        lines = slice(marks[s], marks[s + 1])
        at = pl.ds(marks[s], marks[s + 1] - marks[s])
        acc = kept[s]
        if nz > 1:
            arrived(zr_v.at[pl.ds(1, nz - 1), at, :], "zr", s)
        for q in range(1, nz):
            acc = acc + zr_v[q, lines, :].astype(f32)
        dtok_ref[lines, :] = acc.astype(bf16)

    remote_rows = pl.ds(cap, far)
    for s in range(len(cuts)):
        for i, (a, off, w, shared) in enumerate(plan[s]):
            cols = window(s, i, odd)[1]
            sent(snd_v.at[a, pl.ds(bases[s] - cap, slabs[s]), cols], "ds", 0)
            if shared:
                sent(area(s, i, whole(s), odd), "hs", 0)
    for a in range(2):
        sent(all_v.at[a, core, remote_rows, :], "ys", 0)
    sent(gsnd_v.at[pl.ds(1, ep - 1)], "gs", 0)
    sent(ps_v, "ps", 0)
    sent(xs_v.at[:, remote_rows, :], "xs", 0)
    if nz > 1:
        sent(zs_v.at[pl.ds(1, nz - 1)], "zs", 0)
    sent(gp_v.at[pl.ds(1, tp - 1)], "as", 0)
    sent(gsum_v.at[pl.ds(1, ep - 1)], "bs", 0)
    sent(nr_v.at[pl.ds(1, tp - 1)], "ns", 0)


def write_out(*refs):
    count = (len(refs) - 1) // 2
    copies = [
        pltpu.make_async_copy(refs[i], refs[count + i], refs[-1].at[i]) for i in range(count)
    ]
    for cp in copies:
        cp.start()
    for cp in copies:
        cp.wait()


def shards(tokens, routes, gates, cotangent, w_glu, w_lin, w_down):
    ep = lax.axis_size("ep")
    tp = lax.axis_size("tp")
    rows, top = routes.shape
    width = tokens.shape[1]
    units = w_glu.shape[2]
    cap = 3 * rows * top // (2 * ep)
    cap = -(-cap // 32) * 32
    slots = ep * cap
    half = width // CORES
    own = width // tp
    nz = tp // CORES
    vm = pl.BlockSpec(memory_space=pltpu.VMEM)
    hbm = pl.BlockSpec(memory_space=pltpu.HBM)
    dma = pltpu.SemaphoreType.DMA
    erows = max(8, ep)
    V = pltpu.VMEM
    out_shape = (
        jax.ShapeDtypeStruct((rows, own), bf16),
        jax.ShapeDtypeStruct((top, rows), f32),
        jax.ShapeDtypeStruct((width, units), f32),
        jax.ShapeDtypeStruct((width, units), f32),
        jax.ShapeDtypeStruct((units, width), f32),
        jax.ShapeDtypeStruct((1, width), f32),
        jax.ShapeDtypeStruct((1, width), f32),
        jax.ShapeDtypeStruct((1, units), f32),
    )
    outs = pl.pallas_call(
        functools.partial(kernel, ep, tp, cap),
        out_shape=out_shape,
        in_specs=[hbm] * 7,
        out_specs=(vm,) * 8,
        scratch_shapes=[
            V((rows, width), bf16),
            V((top, rows), jnp.int32),
            V((top, rows), f32),
            V((rows, width), bf16),
            V((width, units) if units % LANES else (16, LANES), bf16),
            V((width, units) if units % LANES else (16, LANES), bf16),
            V((width, 2 * units), bf16),
            V((units, width), bf16),
            V((rows, slots), bf16),
            V((ep, LANES, rows), bf16),
            V((2, slots - cap, half), bf16),
            V((2, CORES, slots, half), bf16),
            V((ep, 8, LANES), f32),
            V((ep, 8, LANES), f32),
            V((slots, 2 * units), bf16),
            V((slots, units), bf16),
            V((3 * units, slots), bf16),
            V((nz, slots, own), bf16),
            V((nz, slots, own), bf16),
            V((nz, slots, own), bf16),
            V((nz, slots, own), bf16),
            V((nz, rows, own), bf16),
            V((nz, rows, own), bf16),
            V((tp, erows, LANES), f32),
            V((ep, 8, LANES), f32),
            V((ep, 8, LANES), f32),
            V((2, width), f32),
            V((tp, 2, width), bf16),
            dma((len(semaphores(ep, nz, piece_list(half))),)),
        ],
        compiler_params=pltpu.CompilerParams(
            collective_id=0, has_side_effects=True, vmem_limit_bytes=28 * 1024 * 1024
        ),
    )(*(pltpu.with_memory_space_constraint(x, pltpu.HBM) for x in (
        tokens, routes.T, gates.T, cotangent, w_glu[0], w_lin[0], w_down[0]
    )))
    outs = pl.pallas_call(
        write_out,
        out_shape=out_shape,
        in_specs=[vm] * len(out_shape),
        out_specs=(hbm,) * len(out_shape),
        scratch_shapes=[dma((len(out_shape),))],
        compiler_params=pltpu.CompilerParams(vmem_limit_bytes=28 * 1024 * 1024),
    )(*outs)
    d_tokens, d_gates, gw, lw, dw, gn, ln, dn = outs
    return (d_tokens, d_gates.T, gw[None], lw[None], dw[None], gn, ln, dn)


def solution(mesh):
    in_specs = (
        P("ep", None),
        P("ep", None),
        P("ep", None),
        P("ep", None),
        P("ep", None, "tp"),
        P("ep", None, "tp"),
        P("ep", "tp", None),
    )
    out_specs = (
        P("ep", "tp"),
        P("ep", None),
        P("ep", None, "tp"),
        P("ep", None, "tp"),
        P("ep", "tp", None),
        P("ep", None),
        P("ep", None),
        P("ep", "tp"),
    )
    return jax.shard_map(shards, mesh=mesh, in_specs=in_specs, out_specs=out_specs, check_vma=False)
```

```python
import functools

import jax
import jax.numpy as jnp
from jax import lax
from jax.experimental import pallas as pl
from jax.experimental.pallas import tpu as pltpu
from jax.sharding import PartitionSpec as P

clamp_limit = 7.0
sigmoid_scale = 1.702
MESH = pl.DeviceIdType.MESH
LANES = 128
CORES = 2
SHARE = 3
FLIGHT = 6
f32 = jnp.float32
bf16 = jnp.bfloat16


def dot_nn(a, b):
    return lax.dot_general(a, b, (((1,), (0,)), ((), ())), preferred_element_type=f32)


def dot_nt(a, b):
    return lax.dot_general(a, b, (((1,), (1,)), ((), ())), preferred_element_type=f32)


def flip(index, mask):
    bit = 1
    while bit <= mask:
        if mask & bit:
            index = index + bit - 2 * bit * lax.rem(lax.div(index, bit), 2)
        bit = 2 * bit
    return index


def clamp_backward(glu_pre, lin_pre, back_proj, gate_col):
    glu_clip = jnp.minimum(glu_pre, clamp_limit)
    lin_clip = jnp.clip(lin_pre, -clamp_limit, clamp_limit)
    sig_val = jax.nn.sigmoid(sigmoid_scale * glu_clip)
    glu_act = glu_clip * sig_val
    hidden = glu_act * (lin_clip + 1.0)
    hid_grad = gate_col * back_proj
    act_slope = sig_val + sigmoid_scale * glu_clip * sig_val * (1.0 - sig_val)
    glu_grad = jnp.where(glu_pre < clamp_limit, hid_grad * (lin_clip + 1.0) * act_slope, 0.0)
    lin_grad = jnp.where(jnp.abs(lin_pre) < clamp_limit, hid_grad * glu_act, 0.0)
    return hidden, glu_grad.astype(bf16), lin_grad.astype(bf16)


def slab_cuts(cap):
    first = min(-(-2 * cap // 48) * 16, cap - 16)
    return (first, cap - first)


def piece_list(half):
    unit = half // 8
    early = tuple((1, 2 * k * unit, unit, True) for k in range(4)) + (
        (0, 0, unit, True),
    ) + tuple((0, (2 + 2 * k) * unit, 2 * unit, False) for k in range(3))
    late = (
        (1, 0, SHARE * unit, True),
        (1, 2 * SHARE * unit, half - 2 * SHARE * unit, False),
        (0, 0, half // 2, False),
        (0, half // 2, half // 2, False),
    )
    return (early, late)


def semaphores(ep, nz, plan):
    keys = [("load", i) for i in range(7)]
    keys += [(k, 0) for k in ("gs", "ps", "xs", "zs", "as", "bs", "ns", "ds", "hs", "ys")]
    keys += [(k, 0) for k in ("gr", "ar", "br", "nr", "ur", "us")]
    for s, pieces in enumerate(plan):
        for i, piece in enumerate(pieces):
            keys.append(("dr", s, i))
            if piece[3]:
                keys.append(("hr", s, i))
        keys += [("yr", s, a) for a in range(2)]
        keys.append(("zr", s))
    for q in range(nz):
        keys += [("pr", q, b) for b in range(1 + len(plan))]
        keys += [("xr", q, s) for s in range(len(plan))]
    return {key: i for i, key in enumerate(keys)}


def kernel(
    ep, tp, cap,
    tok_hbm, routes_hbm, gates_hbm, cot_hbm, wg_hbm, wl_hbm, wd_hbm,
    dtok_ref, dgate_ref, gw_v, lw_v, dw_v, gn_ref, ln_ref, dn_ref,
    tok_ref, routes_ref, gates_ref, cot_ref, wg_ref, wl_ref, wcat_ref, wd_ref,
    pt_v, pk_v, snd_v, all_v, gsnd_v, grow_v, bf_v, hg_v, tr_v,
    ps_v, pr_v, mine_v, xs_v, ret_v, zs_v, zr_v,
    gp_v, gsum_v, gback_v, ns_v, np_v, nr_v, sem_v,
):
    me = lax.axis_index("ep")
    tpi = lax.axis_index("tp")
    nz = tp // CORES
    core = lax.rem(tpi, CORES)
    chip = lax.div(tpi, CORES)
    other = 1 - core
    partner = chip * CORES + other
    rows = tok_ref.shape[0]
    width = tok_ref.shape[1]
    units = wd_ref.shape[0]
    half = width // CORES
    own = width // tp
    odd = lax.rem(chip, 2)
    beside = flip(chip, 1) * CORES + core
    cuts = slab_cuts(cap)
    slabs = [(ep - 1) * n for n in cuts]
    bases = [cap + sum(slabs[:s]) for s in range(len(cuts))]
    ranks = [sum(cuts[:s]) for s in range(len(cuts))]
    far = sum(slabs)
    plan = piece_list(half)
    table = semaphores(ep, nz, plan)

    def sem(*key):
        return sem_v.at[table[key]]

    aligned = units % LANES == 0
    loads = []
    for i, (src, dst) in enumerate((
        (routes_hbm, routes_ref), (gates_hbm, gates_ref), (cot_hbm, cot_ref), (tok_hbm, tok_ref),
        (wg_hbm, wcat_ref.at[:, pl.ds(0, units)] if aligned else wg_ref),
        (wl_hbm, wcat_ref.at[:, pl.ds(units, units)] if aligned else wl_ref),
        (wd_hbm, wd_ref),
    )):
        cp = pltpu.make_async_copy(src, dst, sem("load", i))
        cp.start()
        loads.append(cp)

    barrier = pltpu.get_barrier_semaphore()
    for r in range(1, ep):
        pl.semaphore_signal(barrier, inc=1, device_id={"ep": flip(me, r)}, device_id_type=MESH)
    for q in range(1, tp):
        pl.semaphore_signal(
            barrier, inc=1, device_id={"tp": lax.rem(tpi + q, tp)}, device_id_type=MESH
        )

    def remote(src, dst, ss, rs, where):
        return pltpu.make_async_remote_copy(
            src_ref=src, dst_ref=dst, send_sem=ss, recv_sem=rs,
            device_id=where, device_id_type=MESH,
        )

    def arrived(ref, *key):
        remote(ref, ref, sem(*key), sem(*key), {"tp": partner}).wait_recv()

    def sent(ref, *key):
        remote(ref, ref, sem(*key), sem(*key), {"tp": partner}).wait_send()

    loads[0].wait()
    loads[1].wait()
    rel = jnp.bitwise_xor(routes_ref[...], me)
    erows = max(8, ep)
    sub = lax.broadcasted_iota(jnp.int32, (erows, rows), 0)
    first, second = sub == rel[0:1, :], sub == rel[1:2, :]
    mask = jnp.where(first, 1.0, 0.0) + jnp.where(second, 1.0, 0.0)
    gate_of = jnp.where(first, gates_ref[0:1, :], 0.0) + jnp.where(second, gates_ref[1:2, :], 0.0)
    before = lax.broadcasted_iota(jnp.int32, (rows, rows), 0) < lax.broadcasted_iota(
        jnp.int32, (rows, rows), 1
    )
    rank = dot_nn(mask.astype(bf16), jnp.where(before, 1.0, 0.0).astype(bf16))
    place = jnp.where(mask > 0.5, rank, -1.0)
    slot_at = lax.broadcasted_iota(jnp.int32, (LANES, rows), 0).astype(f32)
    hits = [jnp.where(slot_at == place[r:r + 1, :], 1.0, 0.0) for r in range(ep)]
    outgoing = [
        jnp.concatenate([hits[r][at:at + n, :] for r in range(1, ep)], axis=0)
        for at, n in zip(ranks, cuts)
    ]
    picks = [x.astype(bf16) for x in outgoing]
    square = lax.broadcasted_iota(jnp.int32, (LANES, LANES), 0) == lax.broadcasted_iota(
        jnp.int32, (LANES, LANES), 1
    )
    refs = (tok_ref, cot_ref)

    def window(s, i, whose):
        a, off, w, shared = plan[s][i]
        if shared:
            return a, pl.ds(pl.multiple_of(off + whose * w, LANES), w)
        return a, pl.ds(off, w)

    def block(s, r):
        return pl.ds(bases[s] + (r - 1) * cuts[s], cuts[s])

    def whole(s):
        return pl.ds(bases[s], slabs[s])

    def area(s, i, at, whose):
        a, cols = window(s, i, whose)
        return all_v.at[a, core, at, cols]

    def relay(s, i, whose):
        at = area(s, i, whole(s), whose)
        remote(at, at, sem("ys", 0), sem("yr", s, plan[s][i][0]), {"tp": partner}).start()

    steps = [(s, i) for s in range(len(cuts)) for i in range(len(plan[s]))]
    state = {"next": 0, "load": 0, "waited": False}

    def cost(s, i):
        return cuts[s] * plan[s][i][2]

    def dispatch():
        s, i = steps[state["next"]]
        a, off, w, shared = plan[s][i]
        cols = window(s, i, odd)[1]
        begin = core * half + off + (odd * w if shared else 0)
        src_cols = pl.ds(pl.multiple_of(begin, LANES), w)
        at = bases[s] - cap
        snd_v[a, at:at + slabs[s], cols] = dot_nn(picks[s], refs[a][:, src_cols]).astype(bf16)
        if not state["waited"]:
            pl.semaphore_wait(barrier, ep - 1 + tp - 1)
            state["waited"] = True
        for r in reversed(range(1, ep)):
            remote(
                snd_v.at[a, pl.ds(at + (r - 1) * cuts[s], cuts[s]), cols],
                area(s, i, block(s, r), odd), sem("ds", 0), sem("dr", s, i), {"ep": flip(me, r)},
            ).start()
        state["next"] += 1
        state["load"] += cost(s, i)

    def fill():
        while state["next"] < len(steps) and state["load"] < FLIGHT * cuts[0] * half // 8:
            dispatch()

    def land(s, i):
        at = area(s, i, whole(s), odd)
        arrived(at, "dr", s, i)
        if plan[s][i][3]:
            remote(at, at, sem("hs", 0), sem("hr", s, i), {"tp": beside}).start()
        relay(s, i, odd)
        state["load"] -= cost(s, i)
        fill()

    def turn(s, i):
        arrived(area(s, i, whole(s), 1 - odd), "hr", s, i)
        relay(s, i, 1 - odd)

    loads[2].wait()
    loads[3].wait()
    fill()
    for r in range(ep):
        col = jnp.sum(hits[r] * gate_of[r:r + 1, :], axis=1, keepdims=True)
        row = jnp.sum(jnp.where(square, col, 0.0), axis=0, keepdims=True)
        if r == 0:
            grow_v[0] = jnp.broadcast_to(row, (8, LANES))
        else:
            gsnd_v[r] = jnp.broadcast_to(row, (8, LANES))
            remote(
                gsnd_v.at[r], grow_v.at[r], sem("gs", 0), sem("gr", 0), {"ep": flip(me, r)}
            ).start()
    home = hits[0][:cap, :].astype(bf16)
    for a, ref in ((0, tok_ref), (1, cot_ref)):
        for h in range(CORES):
            all_v[a, h, 0:cap, :] = dot_nn(home, ref[:, h * half:(h + 1) * half]).astype(bf16)
    for r in range(ep):
        pk_v[r] = hits[r].astype(bf16)
    pt_v[...] = jnp.concatenate([hits[0][:cap, :]] + outgoing, axis=0).T.astype(bf16)

    gp_v[tpi] = jnp.zeros(gp_v.shape[1:], f32)

    def forward(at, count, blocks, shift, ready):
        eye = lax.broadcasted_iota(jnp.int32, (count, LANES), 0) + shift == (
            lax.broadcasted_iota(jnp.int32, (count, LANES), 1)
        )
        rs = slice(at, at + count * len(blocks))
        n = rs.stop - rs.start
        ready(1)
        back = jnp.zeros((n, units), f32)
        for h in range(CORES):
            back = back + dot_nt(all_v[1, h, rs, :], wd_ref[:, h * half:(h + 1) * half])
        gate_col = jnp.concatenate([
            jnp.sum(jnp.where(eye, grow_v[r, 0:1, :], 0.0), axis=1, keepdims=True)
            for r in blocks
        ], axis=0)
        ready(0)
        pre = jnp.zeros((n, 2 * units), f32)
        for h in range(CORES):
            pre = pre + dot_nn(all_v[0, h, rs, :], wcat_ref[h * half:(h + 1) * half, :])
        hidden, glu_bf, lin_bf = clamp_backward(
            pre[:, 0:units], pre[:, units:2 * units], back, gate_col
        )
        part = jnp.sum(back * hidden, axis=1, keepdims=True)
        bf_v[rs, 0:units] = glu_bf
        bf_v[rs, units:2 * units] = lin_bf
        hg_v[rs, :] = (gate_col * hidden).astype(bf16)
        for k, r in enumerate(blocks):
            line = jnp.sum(
                jnp.where(eye, part[k * count:(k + 1) * count, :], 0.0), axis=0, keepdims=True
            )
            gp_v[tpi, r:r + 1, :] = gp_v[tpi, r:r + 1, :] + line

    order = list(reversed(range(1, nz))) + [0]

    def input_cols(k, which, rs):
        at = pl.ds(pl.multiple_of((flip(chip, k) * CORES + which) * own, own), own)
        return dot_nt(bf_v[rs, :], wcat_ref[at, :])

    def give(b, rs):
        at = pl.ds(rs.start, rs.stop - rs.start)
        for q in order:
            ps_v[q, rs, :] = input_cols(q, other, rs).astype(bf16)
        for q in order:
            remote(
                ps_v.at[q, at, :], pr_v.at[q, at, :], sem("ps", 0), sem("pr", q, b),
                {"tp": partner},
            ).start()
        for q in order:
            mine_v[q, rs, :] = input_cols(q, core, rs)

    def take(b, rs):
        at = pl.ds(rs.start, rs.stop - rs.start)
        for q in order:
            arrived(pr_v.at[q, at, :], "pr", q, b)
            total = (mine_v[q, rs, :] + pr_v[q, rs, :].astype(f32)).astype(bf16)
            if b == 0:
                ret_v[q, rs, :] = total
                continue
            xs_v[q, rs, :] = total
            for r in reversed(range(1, ep)):
                where = block(b - 1, r)
                remote(
                    xs_v.at[q, where, :], ret_v.at[q, where, :],
                    sem("xs", 0), sem("xr", q, b - 1), {"ep": flip(me, r)},
                ).start()

    def slab_rows(s):
        return slice(bases[s], bases[s] + slabs[s])

    def landed(s):
        def ready(a):
            if a == 0 and s == 0:
                for i in is_shared(1):
                    land(1, i)
            arrived(all_v.at[a, other, whole(s), :], "yr", s, a)
        return ready

    def is_shared(s):
        return [i for i, piece in enumerate(plan[s]) if piece[3]]

    marks = [0, ranks[1], rows]

    def combine(s, which):
        kept = None
        lines = slice(marks[s], marks[s + 1])
        at = pl.ds(marks[s], marks[s + 1] - marks[s])
        deep = bases[s] + slabs[s]
        for q in which:
            arrived(ret_v.at[q, whole(s), :], "xr", q, s)
            part = dot_nn(pt_v[lines, 0:deep], ret_v[q, 0:deep, :])
            if q == 0:
                kept = part
                continue
            zs_v[q, lines, :] = part.astype(bf16)
            remote(
                zs_v.at[q, at, :], zr_v.at[q, at, :], sem("zs", 0), sem("zr", s),
                {"tp": flip(chip, q) * CORES + core},
            ).start()
        return kept

    home_rows = slice(0, cap)
    remote_blocks = list(range(1, ep))
    for cp in loads[4:]:
        cp.wait()
    if not aligned:
        wcat_ref[...] = jnp.concatenate([wg_ref[...], wl_ref[...]], axis=1)
    forward(0, cap, [0], 0, lambda a: None)
    give(0, home_rows)
    lag = 2
    turns = []
    for i in range(len(plan[0])):
        land(0, i)
        if i == 3:
            take(0, home_rows)
        if plan[0][i][3]:
            turns.append(i)
        while len(turns) > lag or (turns and not plan[0][i][3]):
            turn(0, turns.pop(0))
    arrived(grow_v.at[pl.ds(1, ep - 1)], "gr", 0)
    forward(bases[0], cuts[0], remote_blocks, ranks[0], landed(0))
    give(1, slab_rows(0))
    rest = [i for i in range(len(plan[1])) if not plan[1][i][3]]
    take(1, slab_rows(0))
    for i in rest[:-1]:
        land(1, i)
    for i in is_shared(1):
        turn(1, i)
    land(1, rest[-1])
    forward(bases[1], cuts[1], remote_blocks, ranks[1], landed(1))
    give(2, slab_rows(1))
    combine(0, order[:1])
    take(2, slab_rows(1))
    for q in range(1, tp):
        remote(
            gp_v.at[tpi], gp_v.at[tpi], sem("as", 0), sem("ar", 0),
            {"tp": lax.rem(tpi + q, tp)},
        ).start()
    kept = [combine(0, order[1:])]
    tr_v[0:2 * units, :] = bf_v[...].astype(f32).T.astype(bf16)
    tr_v[2 * units:3 * units, :] = hg_v[...].astype(f32).T.astype(bf16)
    step = min(512, half)
    for h in range(CORES):
        for c0 in range(0, half, step):
            cols = slice(h * half + c0, h * half + c0 + step)
            w = dot_nn(tr_v[0:2 * units, :], all_v[0, h, :, c0:c0 + step])
            for n, w_v in enumerate((gw_v, lw_v)):
                wn = w[n * units:(n + 1) * units, :]
                ns_v[n:n + 1, cols] = jnp.sum(wn * wn, axis=0, keepdims=True)
                w_v[cols, :] = wn.T
    remote(ns_v, np_v, sem("us", 0), sem("ur", 0), {"tp": partner}).start()

    norm = jnp.zeros((units, 1), f32)
    for h in range(CORES):
        for c0 in range(0, half, step):
            cols = slice(h * half + c0, h * half + c0 + step)
            w = dot_nn(tr_v[2 * units:3 * units, :], all_v[1, h, :, c0:c0 + step])
            norm = norm + jnp.sum(w * w, axis=1, keepdims=True)
            dw_v[:, cols] = w
    diag = lax.broadcasted_iota(jnp.int32, (units, units), 0) == (
        lax.broadcasted_iota(jnp.int32, (units, units), 1)
    )
    dn_ref[...] = jnp.sum(jnp.where(diag, norm, 0.0), axis=0, keepdims=True)


    arrived(np_v, "ur", 0)
    nr_v[chip] = (ns_v[...] + np_v[...]).astype(bf16)
    mine_cols = pl.ds(pl.multiple_of(core * half, LANES), half)
    for z in range(1, nz):
        for c in range(CORES):
            at = nr_v.at[chip, :, mine_cols]
            remote(
                at, at, sem("ns", 0), sem("nr", 0), {"tp": flip(chip, z) * CORES + c}
            ).start()
    arrived(gp_v.at[pl.ds(1, tp - 1)], "ar", 0)
    gsum = gp_v[0]
    for j in range(1, tp):
        gsum = gsum + gp_v[j]
    gback_v[0, 0:1, :] = gsum[0:1, :]
    for r in range(1, ep):
        gsum_v[r] = jnp.broadcast_to(gsum[r:r + 1, :], (8, LANES))
        remote(
            gsum_v.at[r], gback_v.at[r], sem("bs", 0), sem("br", 0), {"ep": flip(me, r)}
        ).start()
    kept.append(combine(1, order))
    arrived(gback_v.at[pl.ds(1, ep - 1)], "br", 0)
    res = [jnp.zeros((1, rows), f32), jnp.zeros((1, rows), f32)]
    for r in range(ep):
        col = jnp.sum(jnp.where(square, gback_v[r, 0:1, :], 0.0), axis=1, keepdims=True)
        val = jnp.sum(pk_v[r].astype(f32) * col, axis=0, keepdims=True)
        for k in range(2):
            res[k] = res[k] + jnp.where(rel[k:k + 1, :] == r, val, 0.0)
    dgate_ref[0:1, :] = res[0]
    dgate_ref[1:2, :] = res[1]

    if nz > 1:
        arrived(nr_v.at[pl.ds(1, nz - 1)], "nr", 0)
    norms = nr_v[0].astype(f32)
    for j in range(1, nz):
        norms = norms + nr_v[j].astype(f32)
    gn_ref[...] = norms[0:1, :]
    ln_ref[...] = norms[1:2, :]

    for s in range(len(cuts)):
        lines = slice(marks[s], marks[s + 1])
        at = pl.ds(marks[s], marks[s + 1] - marks[s])
        acc = kept[s]
        if nz > 1:
            arrived(zr_v.at[pl.ds(1, nz - 1), at, :], "zr", s)
        for q in range(1, nz):
            acc = acc + zr_v[q, lines, :].astype(f32)
        dtok_ref[lines, :] = acc.astype(bf16)

    remote_rows = pl.ds(cap, far)
    for s in range(len(cuts)):
        for i, (a, off, w, shared) in enumerate(plan[s]):
            cols = window(s, i, odd)[1]
            sent(snd_v.at[a, pl.ds(bases[s] - cap, slabs[s]), cols], "ds", 0)
            if shared:
                sent(area(s, i, whole(s), odd), "hs", 0)
    for a in range(2):
        sent(all_v.at[a, core, remote_rows, :], "ys", 0)
    sent(gsnd_v.at[pl.ds(1, ep - 1)], "gs", 0)
    sent(ps_v, "ps", 0)
    sent(xs_v.at[:, remote_rows, :], "xs", 0)
    if nz > 1:
        sent(zs_v.at[pl.ds(1, nz - 1)], "zs", 0)
    sent(gp_v.at[pl.ds(1, tp - 1)], "as", 0)
    sent(gsum_v.at[pl.ds(1, ep - 1)], "bs", 0)
    sent(ns_v, "us", 0)
    if nz > 1:
        sent(nr_v.at[pl.ds(1, nz - 1)], "ns", 0)


def write_out(*refs):
    count = (len(refs) - 1) // 2
    copies = [
        pltpu.make_async_copy(refs[i], refs[count + i], refs[-1].at[i]) for i in range(count)
    ]
    for cp in copies:
        cp.start()
    for cp in copies:
        cp.wait()


def shards(tokens, routes, gates, cotangent, w_glu, w_lin, w_down):
    ep = lax.axis_size("ep")
    tp = lax.axis_size("tp")
    rows, top = routes.shape
    width = tokens.shape[1]
    units = w_glu.shape[2]
    cap = 3 * rows * top // (2 * ep)
    cap = -(-cap // 32) * 32
    slots = ep * cap
    half = width // CORES
    own = width // tp
    nz = tp // CORES
    vm = pl.BlockSpec(memory_space=pltpu.VMEM)
    hbm = pl.BlockSpec(memory_space=pltpu.HBM)
    dma = pltpu.SemaphoreType.DMA
    V = pltpu.VMEM
    out_shape = (
        jax.ShapeDtypeStruct((rows, own), bf16),
        jax.ShapeDtypeStruct((top, rows), f32),
        jax.ShapeDtypeStruct((width, units), f32),
        jax.ShapeDtypeStruct((width, units), f32),
        jax.ShapeDtypeStruct((units, width), f32),
        jax.ShapeDtypeStruct((1, width), f32),
        jax.ShapeDtypeStruct((1, width), f32),
        jax.ShapeDtypeStruct((1, units), f32),
    )
    outs = pl.pallas_call(
        functools.partial(kernel, ep, tp, cap),
        out_shape=out_shape,
        in_specs=[hbm] * 7,
        out_specs=(vm,) * 8,
        scratch_shapes=[
            V((rows, width), bf16),
            V((top, rows), jnp.int32),
            V((top, rows), f32),
            V((rows, width), bf16),
            V((width, units) if units % LANES else (16, LANES), bf16),
            V((width, units) if units % LANES else (16, LANES), bf16),
            V((width, 2 * units), bf16),
            V((units, width), bf16),
            V((rows, slots), bf16),
            V((ep, LANES, rows), bf16),
            V((2, slots - cap, half), bf16),
            V((2, CORES, slots, half), bf16),
            V((ep, 8, LANES), f32),
            V((ep, 8, LANES), f32),
            V((slots, 2 * units), bf16),
            V((slots, units), bf16),
            V((3 * units, slots), bf16),
            V((nz, slots, own), bf16),
            V((nz, slots, own), bf16),
            V((nz, slots, own), f32),
            V((nz, slots, own), bf16),
            V((nz, slots, own), bf16),
            V((nz, rows, own), bf16),
            V((nz, rows, own), bf16),
            V((tp, ep, LANES), f32),
            V((ep, 8, LANES), f32),
            V((ep, 8, LANES), f32),
            V((2, width), f32),
            V((2, width), f32),
            V((nz, 2, width), bf16),
            dma((len(semaphores(ep, nz, piece_list(half))),)),
        ],
        compiler_params=pltpu.CompilerParams(
            collective_id=0, has_side_effects=True, vmem_limit_bytes=28 * 1024 * 1024
        ),
    )(*(pltpu.with_memory_space_constraint(x, pltpu.HBM) for x in (
        tokens, routes.T, gates.T, cotangent, w_glu[0], w_lin[0], w_down[0]
    )))
    outs = pl.pallas_call(
        write_out,
        out_shape=out_shape,
        in_specs=[vm] * len(out_shape),
        out_specs=(hbm,) * len(out_shape),
        scratch_shapes=[dma((len(out_shape),))],
        compiler_params=pltpu.CompilerParams(vmem_limit_bytes=28 * 1024 * 1024),
    )(*outs)
    d_tokens, d_gates, gw, lw, dw, gn, ln, dn = outs
    return (d_tokens, d_gates.T, gw[None], lw[None], dw[None], gn, ln, dn)


def solution(mesh):
    in_specs = (
        P("ep", None),
        P("ep", None),
        P("ep", None),
        P("ep", None),
        P("ep", None, "tp"),
        P("ep", None, "tp"),
        P("ep", "tp", None),
    )
    out_specs = (
        P("ep", "tp"),
        P("ep", None),
        P("ep", None, "tp"),
        P("ep", None, "tp"),
        P("ep", "tp", None),
        P("ep", None),
        P("ep", None),
        P("ep", "tp"),
    )
    return jax.shard_map(shards, mesh=mesh, in_specs=in_specs, out_specs=out_specs, check_vma=False)
```

```python
import functools

import jax
import jax.numpy as jnp
from jax import lax
from jax.experimental import pallas as pl
from jax.experimental.pallas import tpu as pltpu
from jax.sharding import PartitionSpec as P

clamp_limit = 7.0
sigmoid_scale = 1.702
MESH = pl.DeviceIdType.MESH
LANES = 128
CORES = 2
SHARE = 3
FLIGHT = 8
LATE = 12
FIRST = 4
f32 = jnp.float32
bf16 = jnp.bfloat16


def dot_nn(a, b):
    return lax.dot_general(a, b, (((1,), (0,)), ((), ())), preferred_element_type=f32)


def dot_nt(a, b):
    return lax.dot_general(a, b, (((1,), (1,)), ((), ())), preferred_element_type=f32)


def flip(index, mask):
    bit = 1
    while bit <= mask:
        if mask & bit:
            index = index + bit - 2 * bit * lax.rem(lax.div(index, bit), 2)
        bit = 2 * bit
    return index


def clamp_backward(glu_pre, lin_pre, back_proj, gate_col):
    glu_clip = jnp.minimum(glu_pre, clamp_limit)
    lin_clip = jnp.clip(lin_pre, -clamp_limit, clamp_limit)
    sig_val = jax.nn.sigmoid(sigmoid_scale * glu_clip)
    glu_act = glu_clip * sig_val
    hidden = glu_act * (lin_clip + 1.0)
    hid_grad = gate_col * back_proj
    act_slope = sig_val + sigmoid_scale * glu_clip * sig_val * (1.0 - sig_val)
    glu_grad = jnp.where(glu_pre < clamp_limit, hid_grad * (lin_clip + 1.0) * act_slope, 0.0)
    lin_grad = jnp.where(jnp.abs(lin_pre) < clamp_limit, hid_grad * glu_act, 0.0)
    return hidden, glu_grad.astype(bf16), lin_grad.astype(bf16)


def slab_cuts(cap):
    tiles = cap // 16
    first = min(-(-tiles * FIRST // 6), tiles - 1)
    return (16 * first, 16 * (tiles - first))


def piece_list(half, count):
    unit = half // 8
    early = tuple((1, 2 * k * unit, unit, True) for k in range(4)) + (
        (0, 0, unit, True),
    ) + tuple((0, (2 + 2 * k) * unit, 2 * unit, False) for k in range(3))
    late = (
        (1, 0, SHARE * unit, True),
        (1, 2 * SHARE * unit, half - 2 * SHARE * unit, False),
        (0, 0, half // 2, False),
        (0, half // 2, half // 2, False),
    )
    return (early,) + (late,) * (count - 1)


def semaphores(ep, nz, plan):
    keys = [("load", i) for i in range(7)]
    keys.append(("out", 0))
    keys += [(k, 0) for k in ("gr", "ar", "br", "nr", "ur")]
    for s, pieces in enumerate(plan):
        for i, piece in enumerate(pieces):
            keys.append(("dr", s, i))
            if piece[3]:
                keys.append(("hr", s, i))
        keys += [("yr", s, a) for a in range(2)]
        keys.append(("zr", s))
    for q in range(nz):
        keys += [("pr", q, b) for b in range(1 + len(plan))]
        keys += [("xr", q, s) for s in range(len(plan))]
    return {key: i for i, key in enumerate(keys)}


def kernel(
    ep, tp, cap,
    tok_hbm, routes_hbm, gates_hbm, cot_hbm, wg_hbm, wl_hbm, wd_hbm,
    dtok_ref, dgate_ref, gw_v, lw_v, dw_v, gn_ref, ln_ref, dn_ref,
    tok_ref, routes_ref, gates_ref, cot_ref, wg_ref, wl_ref, wcat_ref, wd_ref,
    pt_v, pk_v, snd_v, all_v, gsnd_v, grow_v, bf_v, hg_v, tr_v,
    ps_v, pr_v, mine_v, xs_v, ret_v, zs_v, zr_v,
    gp_v, gsum_v, gback_v, ns_v, np_v, nr_v, sem_v,
):
    me = lax.axis_index("ep")
    tpi = lax.axis_index("tp")
    nz = tp // CORES
    core = lax.rem(tpi, CORES)
    chip = lax.div(tpi, CORES)
    other = 1 - core
    partner = chip * CORES + other
    rows = tok_ref.shape[0]
    width = tok_ref.shape[1]
    units = wd_ref.shape[0]
    half = width // CORES
    own = width // tp
    odd = lax.rem(chip, 2)
    beside = flip(chip, 1) * CORES + core
    cuts = slab_cuts(cap)
    slabs = [(ep - 1) * n for n in cuts]
    bases = [cap + sum(slabs[:s]) for s in range(len(cuts))]
    ranks = [sum(cuts[:s]) for s in range(len(cuts))]
    far = sum(slabs)
    plan = piece_list(half, len(cuts))
    table = semaphores(ep, nz, plan)

    def sem(*key):
        return sem_v.at[table[key]]

    aligned = units % LANES == 0
    loads = []
    for i, (src, dst) in enumerate((
        (routes_hbm, routes_ref), (gates_hbm, gates_ref), (cot_hbm, cot_ref), (tok_hbm, tok_ref),
        (wg_hbm, wcat_ref.at[:, pl.ds(0, units)] if aligned else wg_ref),
        (wl_hbm, wcat_ref.at[:, pl.ds(units, units)] if aligned else wl_ref),
        (wd_hbm, wd_ref),
    )):
        cp = pltpu.make_async_copy(src, dst, sem("load", i))
        cp.start()
        loads.append(cp)

    barrier = pltpu.get_barrier_semaphore()
    for r in range(1, ep):
        pl.semaphore_signal(barrier, inc=1, device_id={"ep": flip(me, r)}, device_id_type=MESH)
    for q in range(1, tp):
        pl.semaphore_signal(
            barrier, inc=1, device_id={"tp": lax.rem(tpi + q, tp)}, device_id_type=MESH
        )

    def remote(src, dst, ss, rs, where):
        return pltpu.make_async_remote_copy(
            src_ref=src, dst_ref=dst, send_sem=ss, recv_sem=rs,
            device_id=where, device_id_type=MESH,
        )

    def arrived(ref, *key):
        remote(ref, ref, sem(*key), sem(*key), {"tp": partner}).wait_recv()

    def sent(ref, *key):
        remote(ref, ref, sem(*key), sem(*key), {"tp": partner}).wait_send()

    loads[0].wait()
    loads[1].wait()
    rel = jnp.bitwise_xor(routes_ref[...], me)
    erows = max(8, ep)
    sub = lax.broadcasted_iota(jnp.int32, (erows, rows), 0)
    first, second = sub == rel[0:1, :], sub == rel[1:2, :]
    mask = jnp.where(first, 1.0, 0.0) + jnp.where(second, 1.0, 0.0)
    gate_of = jnp.where(first, gates_ref[0:1, :], 0.0) + jnp.where(second, gates_ref[1:2, :], 0.0)
    before = lax.broadcasted_iota(jnp.int32, (rows, rows), 0) < lax.broadcasted_iota(
        jnp.int32, (rows, rows), 1
    )
    rank = dot_nn(mask.astype(bf16), jnp.where(before, 1.0, 0.0).astype(bf16))
    place = jnp.where(mask > 0.5, rank, -1.0)
    slot_at = lax.broadcasted_iota(jnp.int32, (LANES, rows), 0).astype(f32)
    hits = [jnp.where(slot_at == place[r:r + 1, :], 1.0, 0.0) for r in range(ep)]
    outgoing = [
        jnp.concatenate([hits[r][at:at + n, :] for r in range(1, ep)], axis=0)
        for at, n in zip(ranks, cuts)
    ]
    picks = [x.astype(bf16) for x in outgoing]
    square = lax.broadcasted_iota(jnp.int32, (LANES, LANES), 0) == lax.broadcasted_iota(
        jnp.int32, (LANES, LANES), 1
    )
    refs = (tok_ref, cot_ref)

    def window(s, i, whose):
        a, off, w, shared = plan[s][i]
        if shared:
            return a, pl.ds(pl.multiple_of(off + whose * w, LANES), w)
        return a, pl.ds(off, w)

    def block(s, r):
        return pl.ds(bases[s] + (r - 1) * cuts[s], cuts[s])

    def whole(s):
        return pl.ds(bases[s], slabs[s])

    def area(s, i, at, whose):
        a, cols = window(s, i, whose)
        return all_v.at[a, core, at, cols]

    def relay(s, i, whose):
        at = area(s, i, whole(s), whose)
        remote(at, at, sem("out", 0), sem("yr", s, plan[s][i][0]), {"tp": partner}).start()

    steps = [(s, i) for s in range(len(cuts)) for i in range(len(plan[s]))]
    state = {"next": 0, "load": 0, "waited": False}

    def cost(s, i):
        return cuts[s] * plan[s][i][2]

    def dispatch():
        s, i = steps[state["next"]]
        a, off, w, shared = plan[s][i]
        cols = window(s, i, odd)[1]
        begin = core * half + off + (odd * w if shared else 0)
        src_cols = pl.ds(pl.multiple_of(begin, LANES), w)
        at = bases[s] - cap
        snd_v[a, at:at + slabs[s], cols] = dot_nn(picks[s], refs[a][:, src_cols]).astype(bf16)
        if not state["waited"]:
            pl.semaphore_wait(barrier, ep - 1 + tp - 1)
            state["waited"] = True
        for r in reversed(range(1, ep)):
            remote(
                snd_v.at[a, pl.ds(at + (r - 1) * cuts[s], cuts[s]), cols],
                area(s, i, block(s, r), odd), sem("out", 0), sem("dr", s, i), {"ep": flip(me, r)},
            ).start()
        state["next"] += 1
        state["load"] += cost(s, i)

    def limit():
        units = FLIGHT if steps[state["next"]][0] == 0 else LATE
        return units * cuts[0] * half // 8

    def fill():
        while state["next"] < len(steps) and state["load"] < limit():
            dispatch()

    def land(s, i):
        at = area(s, i, whole(s), odd)
        arrived(at, "dr", s, i)
        if plan[s][i][3]:
            remote(at, at, sem("out", 0), sem("hr", s, i), {"tp": beside}).start()
        relay(s, i, odd)
        state["load"] -= cost(s, i)
        fill()

    def turn(s, i):
        arrived(area(s, i, whole(s), 1 - odd), "hr", s, i)
        relay(s, i, 1 - odd)

    loads[2].wait()
    loads[3].wait()
    fill()
    for r in range(ep):
        col = jnp.sum(hits[r] * gate_of[r:r + 1, :], axis=1, keepdims=True)
        row = jnp.sum(jnp.where(square, col, 0.0), axis=0, keepdims=True)
        if r == 0:
            grow_v[0] = jnp.broadcast_to(row, (8, LANES))
        else:
            gsnd_v[r] = jnp.broadcast_to(row, (8, LANES))
            remote(
                gsnd_v.at[r], grow_v.at[r], sem("out", 0), sem("gr", 0), {"ep": flip(me, r)}
            ).start()
    home = hits[0][:cap, :].astype(bf16)
    for a, ref in ((0, tok_ref), (1, cot_ref)):
        for h in range(CORES):
            all_v[a, h, 0:cap, :] = dot_nn(home, ref[:, h * half:(h + 1) * half]).astype(bf16)
    for r in range(ep):
        pk_v[r] = hits[r].astype(bf16)
    pt_v[...] = jnp.concatenate([hits[0][:cap, :]] + outgoing, axis=0).T.astype(bf16)

    gp_v[tpi] = jnp.zeros(gp_v.shape[1:], f32)

    def forward(at, count, blocks, shift, ready):
        eye = lax.broadcasted_iota(jnp.int32, (count, LANES), 0) + shift == (
            lax.broadcasted_iota(jnp.int32, (count, LANES), 1)
        )
        rs = slice(at, at + count * len(blocks))
        n = rs.stop - rs.start
        ready(1)
        back = jnp.zeros((n, units), f32)
        for h in range(CORES):
            back = back + dot_nt(all_v[1, h, rs, :], wd_ref[:, h * half:(h + 1) * half])
        gate_col = jnp.concatenate([
            jnp.sum(jnp.where(eye, grow_v[r, 0:1, :], 0.0), axis=1, keepdims=True)
            for r in blocks
        ], axis=0)
        ready(0)
        pre = jnp.zeros((n, 2 * units), f32)
        for h in range(CORES):
            pre = pre + dot_nn(all_v[0, h, rs, :], wcat_ref[h * half:(h + 1) * half, :])
        hidden, glu_bf, lin_bf = clamp_backward(
            pre[:, 0:units], pre[:, units:2 * units], back, gate_col
        )
        part = jnp.sum(back * hidden, axis=1, keepdims=True)
        bf_v[rs, 0:units] = glu_bf
        bf_v[rs, units:2 * units] = lin_bf
        hg_v[rs, :] = (gate_col * hidden).astype(bf16)
        for k, r in enumerate(blocks):
            line = jnp.sum(
                jnp.where(eye, part[k * count:(k + 1) * count, :], 0.0), axis=0, keepdims=True
            )
            gp_v[tpi, r:r + 1, :] = gp_v[tpi, r:r + 1, :] + line

    order = list(reversed(range(1, nz))) + [0]

    def input_cols(k, which, rs):
        at = pl.ds(pl.multiple_of((flip(chip, k) * CORES + which) * own, own), own)
        return dot_nt(bf_v[rs, :], wcat_ref[at, :])

    def give(b, rs):
        at = pl.ds(rs.start, rs.stop - rs.start)
        for q in order:
            ps_v[q, rs, :] = input_cols(q, other, rs).astype(bf16)
        for q in order:
            remote(
                ps_v.at[q, at, :], pr_v.at[q, at, :], sem("out", 0), sem("pr", q, b),
                {"tp": partner},
            ).start()
        for q in order:
            mine_v[q, rs, :] = input_cols(q, core, rs)

    def take(b, rs):
        at = pl.ds(rs.start, rs.stop - rs.start)
        for q in order:
            arrived(pr_v.at[q, at, :], "pr", q, b)
            total = (mine_v[q, rs, :] + pr_v[q, rs, :].astype(f32)).astype(bf16)
            if b == 0:
                ret_v[q, rs, :] = total
                continue
            xs_v[q, rs, :] = total
            for r in reversed(range(1, ep)):
                where = block(b - 1, r)
                remote(
                    xs_v.at[q, where, :], ret_v.at[q, where, :],
                    sem("out", 0), sem("xr", q, b - 1), {"ep": flip(me, r)},
                ).start()

    def slab_rows(s):
        return slice(bases[s], bases[s] + slabs[s])

    def landed(s):
        def ready(a):
            if a == 0 and s + 1 < len(cuts):
                for i in is_shared(s + 1):
                    land(s + 1, i)
            arrived(all_v.at[a, other, whole(s), :], "yr", s, a)
        return ready

    def is_shared(s):
        return [i for i, piece in enumerate(plan[s]) if piece[3]]

    marks = ranks + [rows]

    def combine(s, which):
        kept = None
        lines = slice(marks[s], marks[s + 1])
        at = pl.ds(marks[s], marks[s + 1] - marks[s])
        deep = bases[s] + slabs[s]
        for q in which:
            arrived(ret_v.at[q, whole(s), :], "xr", q, s)
            part = dot_nn(pt_v[lines, 0:deep], ret_v[q, 0:deep, :])
            if q == 0:
                kept = part
                continue
            zs_v[q, lines, :] = part.astype(bf16)
            remote(
                zs_v.at[q, at, :], zr_v.at[q, at, :], sem("out", 0), sem("zr", s),
                {"tp": flip(chip, q) * CORES + core},
            ).start()
        return kept

    home_rows = slice(0, cap)
    remote_blocks = list(range(1, ep))
    for cp in loads[4:]:
        cp.wait()
    if not aligned:
        wcat_ref[...] = jnp.concatenate([wg_ref[...], wl_ref[...]], axis=1)
    forward(0, cap, [0], 0, lambda a: None)
    give(0, home_rows)
    lag = 2
    turns = []
    for i in range(len(plan[0])):
        land(0, i)
        if i == 3:
            take(0, home_rows)
        if plan[0][i][3]:
            turns.append(i)
        while len(turns) > lag or (turns and not plan[0][i][3]):
            turn(0, turns.pop(0))
    arrived(grow_v.at[pl.ds(1, ep - 1)], "gr", 0)
    last = len(cuts) - 1
    for s in range(last):
        forward(bases[s], cuts[s], remote_blocks, ranks[s], landed(s))
        give(1 + s, slab_rows(s))
        take(1 + s, slab_rows(s))
        rest = [i for i in range(len(plan[s + 1])) if not plan[s + 1][i][3]]
        for i in rest[:-1]:
            land(s + 1, i)
        for i in is_shared(s + 1):
            turn(s + 1, i)
        land(s + 1, rest[-1])
    forward(bases[last], cuts[last], remote_blocks, ranks[last], landed(last))
    for q in range(1, tp):
        remote(
            gp_v.at[tpi], gp_v.at[tpi], sem("out", 0), sem("ar", 0),
            {"tp": lax.rem(tpi + q, tp)},
        ).start()
    give(1 + last, slab_rows(last))
    combine(0, order[:1])
    tr_v[0:2 * units, :] = bf_v[...].astype(f32).T.astype(bf16)
    tr_v[2 * units:3 * units, :] = hg_v[...].astype(f32).T.astype(bf16)
    step = min(512, half)
    for h in range(CORES):
        for c0 in range(0, half, step):
            cols = slice(h * half + c0, h * half + c0 + step)
            w = dot_nn(tr_v[0:2 * units, :], all_v[0, h, :, c0:c0 + step])
            for n, w_v in enumerate((gw_v, lw_v)):
                wn = w[n * units:(n + 1) * units, :]
                ns_v[n:n + 1, cols] = jnp.sum(wn * wn, axis=0, keepdims=True)
                w_v[cols, :] = wn.T
    remote(ns_v, np_v, sem("out", 0), sem("ur", 0), {"tp": partner}).start()
    take(1 + last, slab_rows(last))
    kept = [combine(0, order[1:])]

    norm = jnp.zeros((units, 1), f32)
    for h in range(CORES):
        for c0 in range(0, half, step):
            cols = slice(h * half + c0, h * half + c0 + step)
            w = dot_nn(tr_v[2 * units:3 * units, :], all_v[1, h, :, c0:c0 + step])
            norm = norm + jnp.sum(w * w, axis=1, keepdims=True)
            dw_v[:, cols] = w
    diag = lax.broadcasted_iota(jnp.int32, (units, units), 0) == (
        lax.broadcasted_iota(jnp.int32, (units, units), 1)
    )
    dn_ref[...] = jnp.sum(jnp.where(diag, norm, 0.0), axis=0, keepdims=True)

    arrived(np_v, "ur", 0)
    nr_v[chip] = (ns_v[...] + np_v[...]).astype(bf16)
    mine_cols = pl.ds(pl.multiple_of(core * half, LANES), half)
    for z in range(1, nz):
        for c in range(CORES):
            at = nr_v.at[chip, :, mine_cols]
            remote(
                at, at, sem("out", 0), sem("nr", 0), {"tp": flip(chip, z) * CORES + c}
            ).start()
    arrived(gp_v.at[pl.ds(1, tp - 1)], "ar", 0)
    gsum = gp_v[0]
    for j in range(1, tp):
        gsum = gsum + gp_v[j]
    gback_v[0, 0:1, :] = gsum[0:1, :]
    for r in range(1, ep):
        gsum_v[r] = jnp.broadcast_to(gsum[r:r + 1, :], (8, LANES))
        remote(
            gsum_v.at[r], gback_v.at[r], sem("out", 0), sem("br", 0), {"ep": flip(me, r)}
        ).start()
    for s in range(1, len(cuts)):
        kept.append(combine(s, order))
    arrived(gback_v.at[pl.ds(1, ep - 1)], "br", 0)
    res = [jnp.zeros((1, rows), f32), jnp.zeros((1, rows), f32)]
    for r in range(ep):
        col = jnp.sum(jnp.where(square, gback_v[r, 0:1, :], 0.0), axis=1, keepdims=True)
        val = jnp.sum(pk_v[r].astype(f32) * col, axis=0, keepdims=True)
        for k in range(2):
            res[k] = res[k] + jnp.where(rel[k:k + 1, :] == r, val, 0.0)
    dgate_ref[0:1, :] = res[0]
    dgate_ref[1:2, :] = res[1]

    if nz > 1:
        arrived(nr_v.at[pl.ds(1, nz - 1)], "nr", 0)
    norms = nr_v[0].astype(f32)
    for j in range(1, nz):
        norms = norms + nr_v[j].astype(f32)
    gn_ref[...] = norms[0:1, :]
    ln_ref[...] = norms[1:2, :]

    for s in range(len(cuts)):
        lines = slice(marks[s], marks[s + 1])
        at = pl.ds(marks[s], marks[s + 1] - marks[s])
        acc = kept[s]
        if nz > 1:
            arrived(zr_v.at[pl.ds(1, nz - 1), at, :], "zr", s)
        for q in range(1, nz):
            acc = acc + zr_v[q, lines, :].astype(f32)
        dtok_ref[lines, :] = acc.astype(bf16)

    remote_rows = pl.ds(cap, far)
    for s in range(len(cuts)):
        for i, (a, off, w, shared) in enumerate(plan[s]):
            cols = window(s, i, odd)[1]
            sent(snd_v.at[a, pl.ds(bases[s] - cap, slabs[s]), cols], "out", 0)
            if shared:
                sent(area(s, i, whole(s), odd), "out", 0)
    for a in range(2):
        sent(all_v.at[a, core, remote_rows, :], "out", 0)
    sent(gsnd_v.at[pl.ds(1, ep - 1)], "out", 0)
    sent(ps_v, "out", 0)
    sent(xs_v.at[:, remote_rows, :], "out", 0)
    if nz > 1:
        sent(zs_v.at[pl.ds(1, nz - 1)], "out", 0)
    sent(gp_v.at[pl.ds(1, tp - 1)], "out", 0)
    sent(gsum_v.at[pl.ds(1, ep - 1)], "out", 0)
    sent(ns_v, "out", 0)
    if nz > 1:
        sent(nr_v.at[pl.ds(1, nz - 1)], "out", 0)


def write_out(*refs):
    count = (len(refs) - 1) // 2
    copies = [
        pltpu.make_async_copy(refs[i], refs[count + i], refs[-1].at[i]) for i in range(count)
    ]
    for cp in copies:
        cp.start()
    for cp in copies:
        cp.wait()


def shards(tokens, routes, gates, cotangent, w_glu, w_lin, w_down):
    ep = lax.axis_size("ep")
    tp = lax.axis_size("tp")
    rows, top = routes.shape
    width = tokens.shape[1]
    units = w_glu.shape[2]
    cap = 3 * rows * top // (2 * ep)
    cap = -(-cap // 32) * 32
    slots = ep * cap
    half = width // CORES
    own = width // tp
    nz = tp // CORES
    vm = pl.BlockSpec(memory_space=pltpu.VMEM)
    hbm = pl.BlockSpec(memory_space=pltpu.HBM)
    dma = pltpu.SemaphoreType.DMA
    V = pltpu.VMEM
    out_shape = (
        jax.ShapeDtypeStruct((rows, own), bf16),
        jax.ShapeDtypeStruct((top, rows), f32),
        jax.ShapeDtypeStruct((width, units), f32),
        jax.ShapeDtypeStruct((width, units), f32),
        jax.ShapeDtypeStruct((units, width), f32),
        jax.ShapeDtypeStruct((1, width), f32),
        jax.ShapeDtypeStruct((1, width), f32),
        jax.ShapeDtypeStruct((1, units), f32),
    )
    outs = pl.pallas_call(
        functools.partial(kernel, ep, tp, cap),
        out_shape=out_shape,
        in_specs=[hbm] * 7,
        out_specs=(vm,) * 8,
        scratch_shapes=[
            V((rows, width), bf16),
            V((top, rows), jnp.int32),
            V((top, rows), f32),
            V((rows, width), bf16),
            V((width, units) if units % LANES else (16, LANES), bf16),
            V((width, units) if units % LANES else (16, LANES), bf16),
            V((width, 2 * units), bf16),
            V((units, width), bf16),
            V((rows, slots), bf16),
            V((ep, LANES, rows), bf16),
            V((2, slots - cap, half), bf16),
            V((2, CORES, slots, half), bf16),
            V((ep, 8, LANES), f32),
            V((ep, 8, LANES), f32),
            V((slots, 2 * units), bf16),
            V((slots, units), bf16),
            V((3 * units, slots), bf16),
            V((nz, slots, own), bf16),
            V((nz, slots, own), bf16),
            V((nz, slots, own), f32),
            V((nz, slots, own), bf16),
            V((nz, slots, own), bf16),
            V((nz, rows, own), bf16),
            V((nz, rows, own), bf16),
            V((tp, ep, LANES), f32),
            V((ep, 8, LANES), f32),
            V((ep, 8, LANES), f32),
            V((2, width), f32),
            V((2, width), f32),
            V((nz, 2, width), bf16),
            dma((len(semaphores(ep, nz, piece_list(half, len(slab_cuts(cap))))),)),
        ],
        compiler_params=pltpu.CompilerParams(
            collective_id=0, has_side_effects=True, vmem_limit_bytes=28 * 1024 * 1024
        ),
    )(*(pltpu.with_memory_space_constraint(x, pltpu.HBM) for x in (
        tokens, routes.T, gates.T, cotangent, w_glu[0], w_lin[0], w_down[0]
    )))
    outs = pl.pallas_call(
        write_out,
        out_shape=out_shape,
        in_specs=[vm] * len(out_shape),
        out_specs=(hbm,) * len(out_shape),
        scratch_shapes=[dma((len(out_shape),))],
        compiler_params=pltpu.CompilerParams(vmem_limit_bytes=28 * 1024 * 1024),
    )(*outs)
    d_tokens, d_gates, gw, lw, dw, gn, ln, dn = outs
    return (d_tokens, d_gates.T, gw[None], lw[None], dw[None], gn, ln, dn)


def solution(mesh):
    in_specs = (
        P("ep", None),
        P("ep", None),
        P("ep", None),
        P("ep", None),
        P("ep", None, "tp"),
        P("ep", None, "tp"),
        P("ep", "tp", None),
    )
    out_specs = (
        P("ep", "tp"),
        P("ep", None),
        P("ep", None, "tp"),
        P("ep", None, "tp"),
        P("ep", "tp", None),
        P("ep", None),
        P("ep", None),
        P("ep", "tp"),
    )
    return jax.shard_map(shards, mesh=mesh, in_specs=in_specs, out_specs=out_specs, check_vma=False)
```

```python
import functools

import jax
import jax.numpy as jnp
from jax import lax
from jax.experimental import pallas as pl
from jax.experimental.pallas import tpu as pltpu
from jax.sharding import PartitionSpec as P

clamp_limit = 7.0
sigmoid_scale = 1.702
MESH = pl.DeviceIdType.MESH
LANES = 128
CORES = 2
SHARE = 3
FLIGHT = 8
LATE = 12
FIRST = 4
f32 = jnp.float32
bf16 = jnp.bfloat16


def dot_nn(a, b):
    return lax.dot_general(a, b, (((1,), (0,)), ((), ())), preferred_element_type=f32)


def dot_nt(a, b):
    return lax.dot_general(a, b, (((1,), (1,)), ((), ())), preferred_element_type=f32)


def flip(index, mask):
    bit = 1
    while bit <= mask:
        if mask & bit:
            index = index + bit - 2 * bit * lax.rem(lax.div(index, bit), 2)
        bit = 2 * bit
    return index


def clamp_backward(glu_pre, lin_pre, back_proj, gate_col):
    glu_clip = jnp.minimum(glu_pre, clamp_limit)
    lin_clip = jnp.clip(lin_pre, -clamp_limit, clamp_limit)
    sig_val = jax.nn.sigmoid(sigmoid_scale * glu_clip)
    glu_act = glu_clip * sig_val
    hidden = glu_act * (lin_clip + 1.0)
    hid_grad = gate_col * back_proj
    act_slope = sig_val + sigmoid_scale * glu_clip * sig_val * (1.0 - sig_val)
    glu_grad = jnp.where(glu_pre < clamp_limit, hid_grad * (lin_clip + 1.0) * act_slope, 0.0)
    lin_grad = jnp.where(jnp.abs(lin_pre) < clamp_limit, hid_grad * glu_act, 0.0)
    return hidden, glu_grad.astype(bf16), lin_grad.astype(bf16)


def slab_cuts(cap):
    tiles = cap // 16
    first = min(-(-tiles * FIRST // 6), tiles - 1)
    return (16 * first, 16 * (tiles - first))


def piece_list(half, count):
    unit = half // 8
    early = tuple((1, 2 * k * unit, unit, True) for k in range(4)) + (
        (0, 0, unit, True),
    ) + tuple((0, (2 + 2 * k) * unit, 2 * unit, False) for k in range(2)) + (
        (0, 6 * unit, unit, False), (0, 7 * unit, unit, False),
    )
    late = (
        (1, 0, SHARE * unit, True),
        (1, 2 * SHARE * unit, half - 2 * SHARE * unit, False),
        (0, 0, half // 2, False),
        (0, half // 2, half // 2, False),
    )
    return (early,) + (late,) * (count - 1)


def semaphores(ep, nz, plan):
    keys = [("load", i) for i in range(7)]
    keys.append(("out", 0))
    keys += [(k, 0) for k in ("gr", "ar", "br", "nr", "ur", "dx", "ye")]
    for s, pieces in enumerate(plan):
        for i, piece in enumerate(pieces):
            keys.append(("dr", s, i))
            if piece[3]:
                keys.append(("hr", s, i))
        keys += [("yr", s, a) for a in range(2)]
        keys.append(("zr", s))
    for q in range(nz):
        keys += [("pr", q, b) for b in range(1 + len(plan))]
        keys += [("xr", q, s) for s in range(len(plan))]
    return {key: i for i, key in enumerate(keys)}


def kernel(
    ep, tp, cap,
    tok_hbm, routes_hbm, gates_hbm, cot_hbm, wg_hbm, wl_hbm, wd_hbm,
    dtok_ref, dgate_ref, gw_v, lw_v, dw_v, gn_ref, ln_ref, dn_ref,
    tok_ref, routes_ref, gates_ref, cot_ref, wg_ref, wl_ref, wcat_ref, wd_ref,
    pt_v, pk_v, snd_v, extra_v, all_v, gsnd_v, grow_v, bf_v, hg_v, back_v, tr_v,
    ps_v, pr_v, mine_v, xs_v, ret_v, zs_v, zr_v,
    gp_v, gsum_v, gback_v, ns_v, np_v, nr_v, sem_v,
):
    me = lax.axis_index("ep")
    tpi = lax.axis_index("tp")
    nz = tp // CORES
    core = lax.rem(tpi, CORES)
    chip = lax.div(tpi, CORES)
    other = 1 - core
    partner = chip * CORES + other
    rows = tok_ref.shape[0]
    width = tok_ref.shape[1]
    units = wd_ref.shape[0]
    half = width // CORES
    own = width // tp
    odd = lax.rem(chip, 2)
    beside = flip(chip, 1) * CORES + core
    cuts = slab_cuts(cap)
    slabs = [(ep - 1) * n for n in cuts]
    bases = [cap + sum(slabs[:s]) for s in range(len(cuts))]
    ranks = [sum(cuts[:s]) for s in range(len(cuts))]
    far = sum(slabs)
    plan = piece_list(half, len(cuts))
    table = semaphores(ep, nz, plan)

    def sem(*key):
        return sem_v.at[table[key]]

    aligned = units % LANES == 0
    loads = []
    for i, (src, dst) in enumerate((
        (routes_hbm, routes_ref), (gates_hbm, gates_ref), (cot_hbm, cot_ref), (tok_hbm, tok_ref),
        (wg_hbm, wcat_ref.at[:, pl.ds(0, units)] if aligned else wg_ref),
        (wl_hbm, wcat_ref.at[:, pl.ds(units, units)] if aligned else wl_ref),
        (wd_hbm, wd_ref),
    )):
        cp = pltpu.make_async_copy(src, dst, sem("load", i))
        cp.start()
        loads.append(cp)

    barrier = pltpu.get_barrier_semaphore()
    for r in range(1, ep):
        pl.semaphore_signal(barrier, inc=1, device_id={"ep": flip(me, r)}, device_id_type=MESH)
    for q in range(1, tp):
        pl.semaphore_signal(
            barrier, inc=1, device_id={"tp": lax.rem(tpi + q, tp)}, device_id_type=MESH
        )

    def remote(src, dst, ss, rs, where):
        return pltpu.make_async_remote_copy(
            src_ref=src, dst_ref=dst, send_sem=ss, recv_sem=rs,
            device_id=where, device_id_type=MESH,
        )

    def arrived(ref, *key):
        remote(ref, ref, sem(*key), sem(*key), {"tp": partner}).wait_recv()

    def sent(ref, *key):
        remote(ref, ref, sem(*key), sem(*key), {"tp": partner}).wait_send()

    loads[0].wait()
    loads[1].wait()
    rel = jnp.bitwise_xor(routes_ref[...], me)
    erows = max(8, ep)
    sub = lax.broadcasted_iota(jnp.int32, (erows, rows), 0)
    first, second = sub == rel[0:1, :], sub == rel[1:2, :]
    mask = jnp.where(first, 1.0, 0.0) + jnp.where(second, 1.0, 0.0)
    gate_of = jnp.where(first, gates_ref[0:1, :], 0.0) + jnp.where(second, gates_ref[1:2, :], 0.0)
    before = lax.broadcasted_iota(jnp.int32, (rows, rows), 0) < lax.broadcasted_iota(
        jnp.int32, (rows, rows), 1
    )
    rank = dot_nn(mask.astype(bf16), jnp.where(before, 1.0, 0.0).astype(bf16))
    place = jnp.where(mask > 0.5, rank, -1.0)
    slot_at = lax.broadcasted_iota(jnp.int32, (LANES, rows), 0).astype(f32)
    hits = [jnp.where(slot_at == place[r:r + 1, :], 1.0, 0.0) for r in range(ep)]
    outgoing = [
        jnp.concatenate([hits[r][at:at + n, :] for r in range(1, ep)], axis=0)
        for at, n in zip(ranks, cuts)
    ]
    picks = [x.astype(bf16) for x in outgoing]
    square = lax.broadcasted_iota(jnp.int32, (LANES, LANES), 0) == lax.broadcasted_iota(
        jnp.int32, (LANES, LANES), 1
    )
    refs = (tok_ref, cot_ref)

    def window(s, i, whose):
        a, off, w, shared = plan[s][i]
        if shared:
            return a, pl.ds(pl.multiple_of(off + whose * w, LANES), w)
        return a, pl.ds(off, w)

    def block(s, r):
        return pl.ds(bases[s] + (r - 1) * cuts[s], cuts[s])

    def whole(s):
        return pl.ds(bases[s], slabs[s])

    def area(s, i, at, whose):
        a, cols = window(s, i, whose)
        return all_v.at[a, core, at, cols]

    def relay(s, i, whose):
        at = area(s, i, whole(s), whose)
        remote(at, at, sem("out", 0), sem("yr", s, plan[s][i][0]), {"tp": partner}).start()

    steps = [(s, i) for s in range(len(cuts)) for i in range(len(plan[s]))]
    state = {"next": 0, "load": 0, "waited": False}

    def cost(s, i):
        return cuts[s] * plan[s][i][2]

    lone = len(plan[0]) - 1
    lone_off, lone_w = plan[0][lone][1:3]
    lone_cols = pl.ds(lone_off, lone_w)

    def lone_dispatch():
        @pl.when(core == CORES - 1)
        def _():
            for h, buf in ((CORES - 1, snd_v.at[0, pl.ds(0, slabs[0]), lone_cols]), (0, extra_v)):
                at = h * half + lone_off
                buf[...] = dot_nn(picks[0], tok_ref[:, at:at + lone_w]).astype(bf16)
                for r in reversed(range(1, ep)):
                    key = ("dr", 0, lone) if h else ("dx", 0)
                    remote(
                        buf.at[pl.ds((r - 1) * cuts[0], cuts[0]), :],
                        all_v.at[0, h, block(0, r), lone_cols],
                        sem("out", 0), sem(*key), {"ep": flip(me, r)},
                    ).start()

    def lone_land():
        @pl.when(core == CORES - 1)
        def _():
            for h in reversed(range(CORES)):
                key = ("dr", 0, lone) if h else ("dx", 0)
                at = all_v.at[0, h, whole(0), lone_cols]
                arrived(at, *key)
                to = sem("yr", 0, 0) if h else sem("ye", 0)
                remote(at, at, sem("out", 0), to, {"tp": partner}).start()

    def dispatch():
        s, i = steps[state["next"]]
        a, off, w, shared = plan[s][i]
        if (s, i) == (0, lone):
            lone_dispatch()
            state["next"] += 1
            state["load"] += cost(s, i)
            return
        cols = window(s, i, odd)[1]
        begin = core * half + off + (odd * w if shared else 0)
        src_cols = pl.ds(pl.multiple_of(begin, LANES), w)
        at = bases[s] - cap
        snd_v[a, at:at + slabs[s], cols] = dot_nn(picks[s], refs[a][:, src_cols]).astype(bf16)
        if not state["waited"]:
            pl.semaphore_wait(barrier, ep - 1 + tp - 1)
            state["waited"] = True
        for r in reversed(range(1, ep)):
            remote(
                snd_v.at[a, pl.ds(at + (r - 1) * cuts[s], cuts[s]), cols],
                area(s, i, block(s, r), odd), sem("out", 0), sem("dr", s, i), {"ep": flip(me, r)},
            ).start()
        state["next"] += 1
        state["load"] += cost(s, i)

    def limit():
        units = FLIGHT if steps[state["next"]][0] == 0 else LATE
        return units * cuts[0] * half // 8

    def fill():
        while state["next"] < len(steps) and state["load"] < limit():
            dispatch()

    def land(s, i):
        if (s, i) == (0, lone):
            lone_land()
            state["load"] -= cost(s, i)
            fill()
            return
        at = area(s, i, whole(s), odd)
        arrived(at, "dr", s, i)
        if plan[s][i][3]:
            remote(at, at, sem("out", 0), sem("hr", s, i), {"tp": beside}).start()
        relay(s, i, odd)
        state["load"] -= cost(s, i)
        fill()

    def turn(s, i):
        arrived(area(s, i, whole(s), 1 - odd), "hr", s, i)
        relay(s, i, 1 - odd)

    loads[2].wait()
    loads[3].wait()
    fill()
    for r in range(ep):
        col = jnp.sum(hits[r] * gate_of[r:r + 1, :], axis=1, keepdims=True)
        row = jnp.sum(jnp.where(square, col, 0.0), axis=0, keepdims=True)
        if r == 0:
            grow_v[0] = jnp.broadcast_to(row, (8, LANES))
        else:
            gsnd_v[r] = jnp.broadcast_to(row, (8, LANES))
            remote(
                gsnd_v.at[r], grow_v.at[r], sem("out", 0), sem("gr", 0), {"ep": flip(me, r)}
            ).start()
    home = hits[0][:cap, :].astype(bf16)
    for a, ref in ((0, tok_ref), (1, cot_ref)):
        for h in range(CORES):
            all_v[a, h, 0:cap, :] = dot_nn(home, ref[:, h * half:(h + 1) * half]).astype(bf16)
    for r in range(ep):
        pk_v[r] = hits[r].astype(bf16)
    pt_v[...] = jnp.concatenate([hits[0][:cap, :]] + outgoing, axis=0).T.astype(bf16)

    gp_v[tpi] = jnp.zeros(gp_v.shape[1:], f32)

    def backward_half(at, count, blocks, ready):
        rs = slice(at, at + count * len(blocks))
        ready(1)
        back = jnp.zeros((rs.stop - rs.start, units), f32)
        for h in range(CORES):
            back = back + dot_nt(all_v[1, h, rs, :], wd_ref[:, h * half:(h + 1) * half])
        back_v[rs, :] = back

    def forward(at, count, blocks, shift, ready):
        eye = lax.broadcasted_iota(jnp.int32, (count, LANES), 0) + shift == (
            lax.broadcasted_iota(jnp.int32, (count, LANES), 1)
        )
        rs = slice(at, at + count * len(blocks))
        gate_col = jnp.concatenate([
            jnp.sum(jnp.where(eye, grow_v[r, 0:1, :], 0.0), axis=1, keepdims=True)
            for r in blocks
        ], axis=0)
        mine_at = pl.ds(pl.multiple_of(core * half, LANES), half)
        other_at = pl.ds(pl.multiple_of(other * half, LANES), half)
        ready(0)
        pre = dot_nn(all_v[0, core, rs, :], wcat_ref[mine_at, :])
        pre = pre + dot_nn(all_v[0, other, rs, :], wcat_ref[other_at, :])
        back = back_v[rs, :]
        hidden, glu_bf, lin_bf = clamp_backward(
            pre[:, 0:units], pre[:, units:2 * units], back, gate_col
        )
        part = jnp.sum(back * hidden, axis=1, keepdims=True)
        bf_v[rs, 0:units] = glu_bf
        bf_v[rs, units:2 * units] = lin_bf
        hg_v[rs, :] = (gate_col * hidden).astype(bf16)
        for k, r in enumerate(blocks):
            line = jnp.sum(
                jnp.where(eye, part[k * count:(k + 1) * count, :], 0.0), axis=0, keepdims=True
            )
            gp_v[tpi, r:r + 1, :] = gp_v[tpi, r:r + 1, :] + line

    order = list(reversed(range(1, nz))) + [0]

    def input_cols(k, which, rs):
        at = pl.ds(pl.multiple_of((flip(chip, k) * CORES + which) * own, own), own)
        return dot_nt(bf_v[rs, :], wcat_ref[at, :])

    def give(b, rs):
        at = pl.ds(rs.start, rs.stop - rs.start)
        for q in order:
            ps_v[q, rs, :] = input_cols(q, other, rs).astype(bf16)
        for q in order:
            remote(
                ps_v.at[q, at, :], pr_v.at[q, at, :], sem("out", 0), sem("pr", q, b),
                {"tp": partner},
            ).start()
        for q in order:
            mine_v[q, rs, :] = input_cols(q, core, rs)

    def take(b, rs):
        at = pl.ds(rs.start, rs.stop - rs.start)
        for q in order:
            arrived(pr_v.at[q, at, :], "pr", q, b)
            total = (mine_v[q, rs, :] + pr_v[q, rs, :].astype(f32)).astype(bf16)
            if b == 0:
                ret_v[q, rs, :] = total
                continue
            xs_v[q, rs, :] = total
            for r in reversed(range(1, ep)):
                where = block(b - 1, r)
                remote(
                    xs_v.at[q, where, :], ret_v.at[q, where, :],
                    sem("out", 0), sem("xr", q, b - 1), {"ep": flip(me, r)},
                ).start()

    def slab_rows(s):
        return slice(bases[s], bases[s] + slabs[s])

    def landed(s):
        def ready(a):
            if a == 0 and s + 1 < len(cuts):
                for i in is_shared(s + 1):
                    land(s + 1, i)
            if (s, a) != (0, 0):
                arrived(all_v.at[a, other, whole(s), :], "yr", s, a)
                return

            @pl.when(core == 0)
            def _():
                arrived(all_v.at[0, CORES - 1, whole(0), :], "yr", 0, 0)
                arrived(all_v.at[0, 0, whole(0), lone_cols], "ye", 0)

            @pl.when(core == CORES - 1)
            def _():
                arrived(all_v.at[0, 0, whole(0), pl.ds(0, lone_off)], "yr", 0, 0)
        return ready

    def is_shared(s):
        return [i for i, piece in enumerate(plan[s]) if piece[3]]

    marks = ranks + [rows]

    def combine(s, which):
        kept = None
        lines = slice(marks[s], marks[s + 1])
        at = pl.ds(marks[s], marks[s + 1] - marks[s])
        deep = bases[s] + slabs[s]
        for q in which:
            arrived(ret_v.at[q, whole(s), :], "xr", q, s)
            part = dot_nn(pt_v[lines, 0:deep], ret_v[q, 0:deep, :])
            if q == 0:
                kept = part
                continue
            zs_v[q, lines, :] = part.astype(bf16)
            remote(
                zs_v.at[q, at, :], zr_v.at[q, at, :], sem("out", 0), sem("zr", s),
                {"tp": flip(chip, q) * CORES + core},
            ).start()
        return kept

    home_rows = slice(0, cap)
    remote_blocks = list(range(1, ep))
    for cp in loads[4:]:
        cp.wait()
    if not aligned:
        wcat_ref[...] = jnp.concatenate([wg_ref[...], wl_ref[...]], axis=1)
    backward_half(0, cap, [0], lambda a: None)
    forward(0, cap, [0], 0, lambda a: None)
    give(0, home_rows)
    lag = 2
    turns = []
    for i in range(len(plan[0])):
        land(0, i)
        if i == 3:
            take(0, home_rows)
        if plan[0][i][3]:
            turns.append(i)
        if len(turns) > lag or (turns and not plan[0][i][3]):
            turn(0, turns.pop(0))
    arrived(grow_v.at[pl.ds(1, ep - 1)], "gr", 0)
    assert not turns
    last = len(cuts) - 1
    for s in range(last):
        backward_half(bases[s], cuts[s], remote_blocks, landed(s))
        forward(bases[s], cuts[s], remote_blocks, ranks[s], landed(s))
        give(1 + s, slab_rows(s))
        take(1 + s, slab_rows(s))
        rest = [i for i in range(len(plan[s + 1])) if not plan[s + 1][i][3]]
        for i in rest[:-1]:
            land(s + 1, i)
        for i in is_shared(s + 1):
            turn(s + 1, i)
        land(s + 1, rest[-1])
    backward_half(bases[last], cuts[last], remote_blocks, landed(last))
    forward(bases[last], cuts[last], remote_blocks, ranks[last], landed(last))
    for q in range(1, tp):
        remote(
            gp_v.at[tpi], gp_v.at[tpi], sem("out", 0), sem("ar", 0),
            {"tp": lax.rem(tpi + q, tp)},
        ).start()
    give(1 + last, slab_rows(last))
    combine(0, order[:1])
    tr_v[0:2 * units, :] = bf_v[...].astype(f32).T.astype(bf16)
    tr_v[2 * units:3 * units, :] = hg_v[...].astype(f32).T.astype(bf16)
    step = min(512, half)
    for h in range(CORES):
        for c0 in range(0, half, step):
            cols = slice(h * half + c0, h * half + c0 + step)
            w = dot_nn(tr_v[0:2 * units, :], all_v[0, h, :, c0:c0 + step])
            for n, w_v in enumerate((gw_v, lw_v)):
                wn = w[n * units:(n + 1) * units, :]
                ns_v[n:n + 1, cols] = jnp.sum(wn * wn, axis=0, keepdims=True)
                w_v[cols, :] = wn.T
    remote(ns_v, np_v, sem("out", 0), sem("ur", 0), {"tp": partner}).start()
    take(1 + last, slab_rows(last))
    kept = [combine(0, order[1:])]

    norm = jnp.zeros((units, 1), f32)
    for h in range(CORES):
        for c0 in range(0, half, step):
            cols = slice(h * half + c0, h * half + c0 + step)
            w = dot_nn(tr_v[2 * units:3 * units, :], all_v[1, h, :, c0:c0 + step])
            norm = norm + jnp.sum(w * w, axis=1, keepdims=True)
            dw_v[:, cols] = w
    diag = lax.broadcasted_iota(jnp.int32, (units, units), 0) == (
        lax.broadcasted_iota(jnp.int32, (units, units), 1)
    )
    dn_ref[...] = jnp.sum(jnp.where(diag, norm, 0.0), axis=0, keepdims=True)

    arrived(np_v, "ur", 0)
    nr_v[chip] = (ns_v[...] + np_v[...]).astype(bf16)
    mine_cols = pl.ds(pl.multiple_of(core * half, LANES), half)
    for z in range(1, nz):
        for c in range(CORES):
            at = nr_v.at[chip, :, mine_cols]
            remote(
                at, at, sem("out", 0), sem("nr", 0), {"tp": flip(chip, z) * CORES + c}
            ).start()
    arrived(gp_v.at[pl.ds(1, tp - 1)], "ar", 0)
    gsum = gp_v[0]
    for j in range(1, tp):
        gsum = gsum + gp_v[j]
    gback_v[0, 0:1, :] = gsum[0:1, :]
    for r in range(1, ep):
        gsum_v[r] = jnp.broadcast_to(gsum[r:r + 1, :], (8, LANES))
        remote(
            gsum_v.at[r], gback_v.at[r], sem("out", 0), sem("br", 0), {"ep": flip(me, r)}
        ).start()
    for s in range(1, len(cuts)):
        kept.append(combine(s, order))
    arrived(gback_v.at[pl.ds(1, ep - 1)], "br", 0)
    res = [jnp.zeros((1, rows), f32), jnp.zeros((1, rows), f32)]
    for r in range(ep):
        col = jnp.sum(jnp.where(square, gback_v[r, 0:1, :], 0.0), axis=1, keepdims=True)
        val = jnp.sum(pk_v[r].astype(f32) * col, axis=0, keepdims=True)
        for k in range(2):
            res[k] = res[k] + jnp.where(rel[k:k + 1, :] == r, val, 0.0)
    dgate_ref[0:1, :] = res[0]
    dgate_ref[1:2, :] = res[1]

    if nz > 1:
        arrived(nr_v.at[pl.ds(1, nz - 1)], "nr", 0)
    norms = nr_v[0].astype(f32)
    for j in range(1, nz):
        norms = norms + nr_v[j].astype(f32)
    gn_ref[...] = norms[0:1, :]
    ln_ref[...] = norms[1:2, :]

    for s in range(len(cuts)):
        lines = slice(marks[s], marks[s + 1])
        at = pl.ds(marks[s], marks[s + 1] - marks[s])
        acc = kept[s]
        if nz > 1:
            arrived(zr_v.at[pl.ds(1, nz - 1), at, :], "zr", s)
        for q in range(1, nz):
            acc = acc + zr_v[q, lines, :].astype(f32)
        dtok_ref[lines, :] = acc.astype(bf16)

    remote_rows = pl.ds(cap, far)
    for s in range(len(cuts)):
        for i, (a, off, w, shared) in enumerate(plan[s]):
            if (s, i) == (0, lone):
                continue
            cols = window(s, i, odd)[1]
            sent(snd_v.at[a, pl.ds(bases[s] - cap, slabs[s]), cols], "out", 0)
            if shared:
                sent(area(s, i, whole(s), odd), "out", 0)
    sent(all_v.at[1, core, remote_rows, :], "out", 0)

    @pl.when(core == CORES - 1)
    def _():
        sent(snd_v.at[0, pl.ds(0, slabs[0]), lone_cols], "out", 0)
        sent(extra_v, "out", 0)
        sent(all_v.at[0, CORES - 1, remote_rows, :], "out", 0)
        sent(all_v.at[0, 0, whole(0), lone_cols], "out", 0)

    @pl.when(core == 0)
    def _():
        sent(all_v.at[0, 0, whole(0), pl.ds(0, lone_off)], "out", 0)
        sent(all_v.at[0, 0, whole(1), :], "out", 0)

    sent(gsnd_v.at[pl.ds(1, ep - 1)], "out", 0)
    sent(ps_v, "out", 0)
    sent(xs_v.at[:, remote_rows, :], "out", 0)
    if nz > 1:
        sent(zs_v.at[pl.ds(1, nz - 1)], "out", 0)
    sent(gp_v.at[pl.ds(1, tp - 1)], "out", 0)
    sent(gsum_v.at[pl.ds(1, ep - 1)], "out", 0)
    sent(ns_v, "out", 0)
    if nz > 1:
        sent(nr_v.at[pl.ds(1, nz - 1)], "out", 0)


def write_out(*refs):
    count = (len(refs) - 1) // 2
    copies = [
        pltpu.make_async_copy(refs[i], refs[count + i], refs[-1].at[i]) for i in range(count)
    ]
    for cp in copies:
        cp.start()
    for cp in copies:
        cp.wait()


def shards(tokens, routes, gates, cotangent, w_glu, w_lin, w_down):
    ep = lax.axis_size("ep")
    tp = lax.axis_size("tp")
    rows, top = routes.shape
    width = tokens.shape[1]
    units = w_glu.shape[2]
    cap = 3 * rows * top // (2 * ep)
    cap = -(-cap // 32) * 32
    slots = ep * cap
    half = width // CORES
    own = width // tp
    nz = tp // CORES
    vm = pl.BlockSpec(memory_space=pltpu.VMEM)
    hbm = pl.BlockSpec(memory_space=pltpu.HBM)
    dma = pltpu.SemaphoreType.DMA
    V = pltpu.VMEM
    out_shape = (
        jax.ShapeDtypeStruct((rows, own), bf16),
        jax.ShapeDtypeStruct((top, rows), f32),
        jax.ShapeDtypeStruct((width, units), f32),
        jax.ShapeDtypeStruct((width, units), f32),
        jax.ShapeDtypeStruct((units, width), f32),
        jax.ShapeDtypeStruct((1, width), f32),
        jax.ShapeDtypeStruct((1, width), f32),
        jax.ShapeDtypeStruct((1, units), f32),
    )
    outs = pl.pallas_call(
        functools.partial(kernel, ep, tp, cap),
        out_shape=out_shape,
        in_specs=[hbm] * 7,
        out_specs=(vm,) * 8,
        scratch_shapes=[
            V((rows, width), bf16),
            V((top, rows), jnp.int32),
            V((top, rows), f32),
            V((rows, width), bf16),
            V((width, units) if units % LANES else (16, LANES), bf16),
            V((width, units) if units % LANES else (16, LANES), bf16),
            V((width, 2 * units), bf16),
            V((units, width), bf16),
            V((rows, slots), bf16),
            V((ep, LANES, rows), bf16),
            V((2, slots - cap, half), bf16),
            V(((ep - 1) * slab_cuts(cap)[0], half // 8), bf16),
            V((2, CORES, slots, half), bf16),
            V((ep, 8, LANES), f32),
            V((ep, 8, LANES), f32),
            V((slots, 2 * units), bf16),
            V((slots, units), bf16),
            V((slots, units), f32),
            V((3 * units, slots), bf16),
            V((nz, slots, own), bf16),
            V((nz, slots, own), bf16),
            V((nz, slots, own), f32),
            V((nz, slots, own), bf16),
            V((nz, slots, own), bf16),
            V((nz, rows, own), bf16),
            V((nz, rows, own), bf16),
            V((tp, ep, LANES), f32),
            V((ep, 8, LANES), f32),
            V((ep, 8, LANES), f32),
            V((2, width), f32),
            V((2, width), f32),
            V((nz, 2, width), bf16),
            dma((len(semaphores(ep, nz, piece_list(half, len(slab_cuts(cap))))),)),
        ],
        compiler_params=pltpu.CompilerParams(
            collective_id=0, has_side_effects=True, vmem_limit_bytes=28 * 1024 * 1024
        ),
    )(*(pltpu.with_memory_space_constraint(x, pltpu.HBM) for x in (
        tokens, routes.T, gates.T, cotangent, w_glu[0], w_lin[0], w_down[0]
    )))
    outs = pl.pallas_call(
        write_out,
        out_shape=out_shape,
        in_specs=[vm] * len(out_shape),
        out_specs=(hbm,) * len(out_shape),
        scratch_shapes=[dma((len(out_shape),))],
        compiler_params=pltpu.CompilerParams(vmem_limit_bytes=28 * 1024 * 1024),
    )(*outs)
    d_tokens, d_gates, gw, lw, dw, gn, ln, dn = outs
    return (d_tokens, d_gates.T, gw[None], lw[None], dw[None], gn, ln, dn)


def solution(mesh):
    in_specs = (
        P("ep", None),
        P("ep", None),
        P("ep", None),
        P("ep", None),
        P("ep", None, "tp"),
        P("ep", None, "tp"),
        P("ep", "tp", None),
    )
    out_specs = (
        P("ep", "tp"),
        P("ep", None),
        P("ep", None, "tp"),
        P("ep", None, "tp"),
        P("ep", "tp", None),
        P("ep", None),
        P("ep", None),
        P("ep", "tp"),
    )
    return jax.shard_map(shards, mesh=mesh, in_specs=in_specs, out_specs=out_specs, check_vma=False)
```

```python
import functools

import jax
import jax.numpy as jnp
from jax import lax
from jax.experimental import pallas as pl
from jax.experimental.pallas import tpu as pltpu
from jax.sharding import PartitionSpec as P

clamp_limit = 7.0
sigmoid_scale = 1.702
MESH = pl.DeviceIdType.MESH
LANES = 128
CORES = 2
SHARE = 3
FLIGHT = 8
LATE = 12
EARLY = 1
FIRST = 4
f32 = jnp.float32
bf16 = jnp.bfloat16


def dot_nn(a, b):
    return lax.dot_general(a, b, (((1,), (0,)), ((), ())), preferred_element_type=f32)


def dot_nt(a, b):
    return lax.dot_general(a, b, (((1,), (1,)), ((), ())), preferred_element_type=f32)


def flip(index, mask):
    bit = 1
    while bit <= mask:
        if mask & bit:
            index = index + bit - 2 * bit * lax.rem(lax.div(index, bit), 2)
        bit = 2 * bit
    return index


def clamp_backward(glu_pre, lin_pre, back_proj, gate_col):
    glu_clip = jnp.minimum(glu_pre, clamp_limit)
    lin_clip = jnp.clip(lin_pre, -clamp_limit, clamp_limit)
    sig_val = jax.nn.sigmoid(sigmoid_scale * glu_clip)
    glu_act = glu_clip * sig_val
    hidden = glu_act * (lin_clip + 1.0)
    hid_grad = gate_col * back_proj
    act_slope = sig_val + sigmoid_scale * glu_clip * sig_val * (1.0 - sig_val)
    glu_grad = jnp.where(glu_pre < clamp_limit, hid_grad * (lin_clip + 1.0) * act_slope, 0.0)
    lin_grad = jnp.where(jnp.abs(lin_pre) < clamp_limit, hid_grad * glu_act, 0.0)
    return hidden, glu_grad.astype(bf16), lin_grad.astype(bf16)


def slab_cuts(cap):
    tiles = cap // 16
    first = min(-(-tiles * FIRST // 6), tiles - 1)
    return (16 * first, 16 * (tiles - first))


def piece_list(half, count):
    unit = half // 8
    early = tuple((1, 2 * k * unit, unit, True) for k in range(4)) + (
        (0, 0, unit, True),
    ) + tuple((0, (2 + 2 * k) * unit, 2 * unit, False) for k in range(2)) + (
        (0, 6 * unit, unit, False), (0, 7 * unit, unit, False),
    )
    late = (
        (1, 0, SHARE * unit, True),
        (1, 2 * SHARE * unit, half - 2 * SHARE * unit, False),
        (0, 0, half // 2, False),
        (0, half // 2, half // 2, False),
    )
    return (early,) + (late,) * (count - 1)


def semaphores(ep, nz, plan):
    keys = [("load", i) for i in range(7)]
    keys.append(("out", 0))
    keys += [(k, 0) for k in ("gr", "ar", "br", "nr", "ur", "dx", "ye")]
    for s, pieces in enumerate(plan):
        for i, piece in enumerate(pieces):
            keys.append(("dr", s, i))
            if piece[3]:
                keys.append(("hr", s, i))
        keys += [("yr", s, a) for a in range(2)]
        keys.append(("zr", s))
    for q in range(nz):
        keys += [("pr", q, b) for b in range(1 + len(plan))]
        keys += [("xr", q, s) for s in range(len(plan))]
    return {key: i for i, key in enumerate(keys)}


def kernel(
    ep, tp, cap,
    tok_hbm, routes_hbm, gates_hbm, cot_hbm, wg_hbm, wl_hbm, wd_hbm,
    dtok_ref, dgate_ref, gw_v, lw_v, dw_v, gn_ref, ln_ref, dn_ref,
    tok_ref, routes_ref, gates_ref, cot_ref, wg_ref, wl_ref, wcat_ref, wd_ref,
    pt_v, pk_v, snd_v, extra_v, all_v, gsnd_v, grow_v, bf_v, hg_v, back_v, tr_v,
    ps_v, pr_v, mine_v, xs_v, ret_v, zs_v, zr_v,
    gp_v, gsum_v, gback_v, ns_v, np_v, nr_v, sem_v,
):
    me = lax.axis_index("ep")
    tpi = lax.axis_index("tp")
    nz = tp // CORES
    core = lax.rem(tpi, CORES)
    chip = lax.div(tpi, CORES)
    other = 1 - core
    partner = chip * CORES + other
    rows = tok_ref.shape[0]
    width = tok_ref.shape[1]
    units = wd_ref.shape[0]
    half = width // CORES
    own = width // tp
    odd = lax.rem(chip, 2)
    beside = flip(chip, 1) * CORES + core
    cuts = slab_cuts(cap)
    slabs = [(ep - 1) * n for n in cuts]
    bases = [cap + sum(slabs[:s]) for s in range(len(cuts))]
    ranks = [sum(cuts[:s]) for s in range(len(cuts))]
    far = sum(slabs)
    plan = piece_list(half, len(cuts))
    table = semaphores(ep, nz, plan)

    def sem(*key):
        return sem_v.at[table[key]]

    aligned = units % LANES == 0
    loads = []
    for i, (src, dst) in enumerate((
        (routes_hbm, routes_ref), (gates_hbm, gates_ref), (cot_hbm, cot_ref), (tok_hbm, tok_ref),
        (wg_hbm, wcat_ref.at[:, pl.ds(0, units)] if aligned else wg_ref),
        (wl_hbm, wcat_ref.at[:, pl.ds(units, units)] if aligned else wl_ref),
        (wd_hbm, wd_ref),
    )):
        cp = pltpu.make_async_copy(src, dst, sem("load", i))
        cp.start()
        loads.append(cp)

    barrier = pltpu.get_barrier_semaphore()
    for r in range(1, ep):
        pl.semaphore_signal(barrier, inc=1, device_id={"ep": flip(me, r)}, device_id_type=MESH)
    for q in range(1, tp):
        pl.semaphore_signal(
            barrier, inc=1, device_id={"tp": lax.rem(tpi + q, tp)}, device_id_type=MESH
        )

    def remote(src, dst, ss, rs, where):
        return pltpu.make_async_remote_copy(
            src_ref=src, dst_ref=dst, send_sem=ss, recv_sem=rs,
            device_id=where, device_id_type=MESH,
        )

    def arrived(ref, *key):
        remote(ref, ref, sem(*key), sem(*key), {"tp": partner}).wait_recv()

    def sent(ref, *key):
        remote(ref, ref, sem(*key), sem(*key), {"tp": partner}).wait_send()

    loads[0].wait()
    loads[1].wait()
    rel = jnp.bitwise_xor(routes_ref[...], me)
    erows = max(8, ep)
    sub = lax.broadcasted_iota(jnp.int32, (erows, rows), 0)
    first, second = sub == rel[0:1, :], sub == rel[1:2, :]
    mask = jnp.where(first, 1.0, 0.0) + jnp.where(second, 1.0, 0.0)
    gate_of = jnp.where(first, gates_ref[0:1, :], 0.0) + jnp.where(second, gates_ref[1:2, :], 0.0)
    before = lax.broadcasted_iota(jnp.int32, (rows, rows), 0) < lax.broadcasted_iota(
        jnp.int32, (rows, rows), 1
    )
    rank = dot_nn(mask.astype(bf16), jnp.where(before, 1.0, 0.0).astype(bf16))
    place = jnp.where(mask > 0.5, rank, -1.0)
    slot_at = lax.broadcasted_iota(jnp.int32, (LANES, rows), 0).astype(f32)
    hits = [jnp.where(slot_at == place[r:r + 1, :], 1.0, 0.0) for r in range(ep)]
    outgoing = [
        jnp.concatenate([hits[r][at:at + n, :] for r in range(1, ep)], axis=0)
        for at, n in zip(ranks, cuts)
    ]
    picks = [x.astype(bf16) for x in outgoing]
    square = lax.broadcasted_iota(jnp.int32, (LANES, LANES), 0) == lax.broadcasted_iota(
        jnp.int32, (LANES, LANES), 1
    )
    refs = (tok_ref, cot_ref)

    def window(s, i, whose):
        a, off, w, shared = plan[s][i]
        if shared:
            return a, pl.ds(pl.multiple_of(off + whose * w, LANES), w)
        return a, pl.ds(off, w)

    def block(s, r):
        return pl.ds(bases[s] + (r - 1) * cuts[s], cuts[s])

    def whole(s):
        return pl.ds(bases[s], slabs[s])

    def area(s, i, at, whose):
        a, cols = window(s, i, whose)
        return all_v.at[a, core, at, cols]

    def relay(s, i, whose):
        at = area(s, i, whole(s), whose)
        remote(at, at, sem("out", 0), sem("yr", s, plan[s][i][0]), {"tp": partner}).start()

    steps = [(s, i) for s in range(len(cuts)) for i in range(len(plan[s]))]
    state = {"next": 0, "load": 0, "waited": False}

    def cost(s, i):
        return cuts[s] * plan[s][i][2]

    lone = len(plan[0]) - 1
    lone_off, lone_w = plan[0][lone][1:3]
    lone_cols = pl.ds(lone_off, lone_w)

    def lone_dispatch():
        @pl.when(core == CORES - 1)
        def _():
            for h, buf in ((CORES - 1, snd_v.at[0, pl.ds(0, slabs[0]), lone_cols]), (0, extra_v)):
                at = h * half + lone_off
                buf[...] = dot_nn(picks[0], tok_ref[:, at:at + lone_w]).astype(bf16)
                for r in reversed(range(1, ep)):
                    key = ("dr", 0, lone) if h else ("dx", 0)
                    remote(
                        buf.at[pl.ds((r - 1) * cuts[0], cuts[0]), :],
                        all_v.at[0, h, block(0, r), lone_cols],
                        sem("out", 0), sem(*key), {"ep": flip(me, r)},
                    ).start()

    def lone_land():
        @pl.when(core == CORES - 1)
        def _():
            for h in reversed(range(CORES)):
                key = ("dr", 0, lone) if h else ("dx", 0)
                at = all_v.at[0, h, whole(0), lone_cols]
                arrived(at, *key)
                to = sem("yr", 0, 0) if h else sem("ye", 0)
                remote(at, at, sem("out", 0), to, {"tp": partner}).start()

    def dispatch():
        s, i = steps[state["next"]]
        a, off, w, shared = plan[s][i]
        if (s, i) == (0, lone):
            lone_dispatch()
            state["next"] += 1
            state["load"] += cost(s, i)
            return
        cols = window(s, i, odd)[1]
        begin = core * half + off + (odd * w if shared else 0)
        src_cols = pl.ds(pl.multiple_of(begin, LANES), w)
        at = bases[s] - cap
        snd_v[a, at:at + slabs[s], cols] = dot_nn(picks[s], refs[a][:, src_cols]).astype(bf16)
        if not state["waited"]:
            pl.semaphore_wait(barrier, ep - 1 + tp - 1)
            state["waited"] = True
        for r in reversed(range(1, ep)):
            remote(
                snd_v.at[a, pl.ds(at + (r - 1) * cuts[s], cuts[s]), cols],
                area(s, i, block(s, r), odd), sem("out", 0), sem("dr", s, i), {"ep": flip(me, r)},
            ).start()
        state["next"] += 1
        state["load"] += cost(s, i)

    def limit():
        units = FLIGHT if steps[state["next"]][0] == 0 else LATE
        return units * cuts[0] * half // 8

    def fill():
        while state["next"] < len(steps) and state["load"] < limit():
            dispatch()

    def land(s, i):
        if (s, i) == (0, lone):
            lone_land()
            state["load"] -= cost(s, i)
            fill()
            return
        at = area(s, i, whole(s), odd)
        arrived(at, "dr", s, i)
        if plan[s][i][3]:
            remote(at, at, sem("out", 0), sem("hr", s, i), {"tp": beside}).start()
        relay(s, i, odd)
        state["load"] -= cost(s, i)
        fill()

    def turn(s, i):
        arrived(area(s, i, whole(s), 1 - odd), "hr", s, i)
        relay(s, i, 1 - odd)

    loads[2].wait()
    loads[3].wait()
    fill()
    for r in range(ep):
        col = jnp.sum(hits[r] * gate_of[r:r + 1, :], axis=1, keepdims=True)
        row = jnp.sum(jnp.where(square, col, 0.0), axis=0, keepdims=True)
        if r == 0:
            grow_v[0] = jnp.broadcast_to(row, (8, LANES))
        else:
            gsnd_v[r] = jnp.broadcast_to(row, (8, LANES))
            remote(
                gsnd_v.at[r], grow_v.at[r], sem("out", 0), sem("gr", 0), {"ep": flip(me, r)}
            ).start()
    home = hits[0][:cap, :].astype(bf16)
    for a, ref in ((0, tok_ref), (1, cot_ref)):
        for h in range(CORES):
            all_v[a, h, 0:cap, :] = dot_nn(home, ref[:, h * half:(h + 1) * half]).astype(bf16)
    for r in range(ep):
        pk_v[r] = hits[r].astype(bf16)
    pt_v[...] = jnp.concatenate([hits[0][:cap, :]] + outgoing, axis=0).T.astype(bf16)

    gp_v[tpi] = jnp.zeros(gp_v.shape[1:], f32)

    def backward_half(at, count, blocks, ready):
        rs = slice(at, at + count * len(blocks))
        ready(1)
        back = jnp.zeros((rs.stop - rs.start, units), f32)
        for h in range(CORES):
            back = back + dot_nt(all_v[1, h, rs, :], wd_ref[:, h * half:(h + 1) * half])
        back_v[rs, :] = back

    def forward(at, count, blocks, shift, ready):
        eye = lax.broadcasted_iota(jnp.int32, (count, LANES), 0) + shift == (
            lax.broadcasted_iota(jnp.int32, (count, LANES), 1)
        )
        rs = slice(at, at + count * len(blocks))
        gate_col = jnp.concatenate([
            jnp.sum(jnp.where(eye, grow_v[r, 0:1, :], 0.0), axis=1, keepdims=True)
            for r in blocks
        ], axis=0)
        mine_at = pl.ds(pl.multiple_of(core * half, LANES), half)
        other_at = pl.ds(pl.multiple_of(other * half, LANES), half)
        ready(0)
        pre = dot_nn(all_v[0, core, rs, :], wcat_ref[mine_at, :])
        pre = pre + dot_nn(all_v[0, other, rs, :], wcat_ref[other_at, :])
        back = back_v[rs, :]
        hidden, glu_bf, lin_bf = clamp_backward(
            pre[:, 0:units], pre[:, units:2 * units], back, gate_col
        )
        part = jnp.sum(back * hidden, axis=1, keepdims=True)
        bf_v[rs, 0:units] = glu_bf
        bf_v[rs, units:2 * units] = lin_bf
        hg_v[rs, :] = (gate_col * hidden).astype(bf16)
        for k, r in enumerate(blocks):
            line = jnp.sum(
                jnp.where(eye, part[k * count:(k + 1) * count, :], 0.0), axis=0, keepdims=True
            )
            gp_v[tpi, r:r + 1, :] = gp_v[tpi, r:r + 1, :] + line

    order = list(reversed(range(1, nz))) + [0]

    def input_cols(k, which, rs):
        at = pl.ds(pl.multiple_of((flip(chip, k) * CORES + which) * own, own), own)
        return dot_nt(bf_v[rs, :], wcat_ref[at, :])

    def give(b, rs):
        at = pl.ds(rs.start, rs.stop - rs.start)
        for q in order:
            ps_v[q, rs, :] = input_cols(q, other, rs).astype(bf16)
        for q in order:
            remote(
                ps_v.at[q, at, :], pr_v.at[q, at, :], sem("out", 0), sem("pr", q, b),
                {"tp": partner},
            ).start()
        for q in order:
            mine_v[q, rs, :] = input_cols(q, core, rs)

    def take(b, rs):
        at = pl.ds(rs.start, rs.stop - rs.start)
        for q in order:
            arrived(pr_v.at[q, at, :], "pr", q, b)
            total = (mine_v[q, rs, :] + pr_v[q, rs, :].astype(f32)).astype(bf16)
            if b == 0:
                ret_v[q, rs, :] = total
                continue
            xs_v[q, rs, :] = total
            for r in reversed(range(1, ep)):
                where = block(b - 1, r)
                remote(
                    xs_v.at[q, where, :], ret_v.at[q, where, :],
                    sem("out", 0), sem("xr", q, b - 1), {"ep": flip(me, r)},
                ).start()

    def slab_rows(s):
        return slice(bases[s], bases[s] + slabs[s])

    def landed(s):
        def ready(a):
            if a == 0 and s + 1 < len(cuts):
                for i in is_shared(s + 1):
                    land(s + 1, i)
            if (s, a) != (0, 0):
                arrived(all_v.at[a, other, whole(s), :], "yr", s, a)
                return

            @pl.when(core == 0)
            def _():
                arrived(all_v.at[0, CORES - 1, whole(0), :], "yr", 0, 0)
                arrived(all_v.at[0, 0, whole(0), lone_cols], "ye", 0)

            @pl.when(core == CORES - 1)
            def _():
                arrived(all_v.at[0, 0, whole(0), pl.ds(0, lone_off)], "yr", 0, 0)
        return ready

    def is_shared(s):
        return [i for i, piece in enumerate(plan[s]) if piece[3]]

    marks = ranks + [rows]

    def combine(s, which):
        kept = None
        lines = slice(marks[s], marks[s + 1])
        at = pl.ds(marks[s], marks[s + 1] - marks[s])
        deep = bases[s] + slabs[s]
        for q in which:
            arrived(ret_v.at[q, whole(s), :], "xr", q, s)
            part = dot_nn(pt_v[lines, 0:deep], ret_v[q, 0:deep, :])
            if q == 0:
                kept = part
                continue
            zs_v[q, lines, :] = part.astype(bf16)
            remote(
                zs_v.at[q, at, :], zr_v.at[q, at, :], sem("out", 0), sem("zr", s),
                {"tp": flip(chip, q) * CORES + core},
            ).start()
        return kept

    home_rows = slice(0, cap)
    remote_blocks = list(range(1, ep))
    for cp in loads[4:]:
        cp.wait()
    if not aligned:
        wcat_ref[...] = jnp.concatenate([wg_ref[...], wl_ref[...]], axis=1)
    backward_half(0, cap, [0], lambda a: None)
    forward(0, cap, [0], 0, lambda a: None)
    give(0, home_rows)
    lag = 2
    turns = []
    for i in range(len(plan[0])):
        land(0, i)
        if i == 3:
            take(0, home_rows)
        if plan[0][i][3]:
            turns.append(i)
        if len(turns) > lag or (turns and not plan[0][i][3]):
            turn(0, turns.pop(0))
    arrived(grow_v.at[pl.ds(1, ep - 1)], "gr", 0)
    last = len(cuts) - 1
    step = min(512, half)

    def turned():
        tr_v[0:2 * units, :] = bf_v[...].astype(f32).T.astype(bf16)
        tr_v[2 * units:3 * units, :] = hg_v[...].astype(f32).T.astype(bf16)

    def up_wgrad(h):
        for c0 in range(0, half, step):
            cols = slice(h * half + c0, h * half + c0 + step)
            w = dot_nn(tr_v[0:2 * units, :], all_v[0, h, :, c0:c0 + step])
            for n, w_v in enumerate((gw_v, lw_v)):
                wn = w[n * units:(n + 1) * units, :]
                ns_v[n:n + 1, cols] = jnp.sum(wn * wn, axis=0, keepdims=True)
                w_v[cols, :] = wn.T

    def down_wgrad(h):
        norm = jnp.zeros((units, 1), f32)
        for c0 in range(0, half, step):
            cols = slice(h * half + c0, h * half + c0 + step)
            w = dot_nn(tr_v[2 * units:3 * units, :], all_v[1, h, :, c0:c0 + step])
            norm = norm + jnp.sum(w * w, axis=1, keepdims=True)
            dw_v[:, cols] = w
        return norm

    for s in range(last):
        backward_half(bases[s], cuts[s], remote_blocks, landed(s))
        forward(bases[s], cuts[s], remote_blocks, ranks[s], landed(s))
        give(1 + s, slab_rows(s))
        rest = [i for i in range(len(plan[s + 1])) if not plan[s + 1][i][3]]
        for i in rest[:EARLY]:
            land(s + 1, i)
        take(1 + s, slab_rows(s))
        for i in rest[EARLY:-1]:
            land(s + 1, i)
        for i in is_shared(s + 1):
            turn(s + 1, i)
        land(s + 1, rest[-1])
    backward_half(bases[last], cuts[last], remote_blocks, landed(last))
    forward(bases[last], cuts[last], remote_blocks, ranks[last], landed(last))
    for q in range(1, tp):
        remote(
            gp_v.at[tpi], gp_v.at[tpi], sem("out", 0), sem("ar", 0),
            {"tp": lax.rem(tpi + q, tp)},
        ).start()
    give(1 + last, slab_rows(last))
    turned()
    up_wgrad(0)
    take(1 + last, slab_rows(last))
    combine(0, order[0:1])
    up_wgrad(1)
    remote(ns_v, np_v, sem("out", 0), sem("ur", 0), {"tp": partner}).start()
    kept = [combine(0, order[1:])]
    diag = lax.broadcasted_iota(jnp.int32, (units, units), 0) == (
        lax.broadcasted_iota(jnp.int32, (units, units), 1)
    )
    norm = down_wgrad(0) + down_wgrad(1)
    dn_ref[...] = jnp.sum(jnp.where(diag, norm, 0.0), axis=0, keepdims=True)
    arrived(np_v, "ur", 0)
    nr_v[chip] = (ns_v[...] + np_v[...]).astype(bf16)
    mine_cols = pl.ds(pl.multiple_of(core * half, LANES), half)
    for z in range(1, nz):
        for c in range(CORES):
            at = nr_v.at[chip, :, mine_cols]
            remote(
                at, at, sem("out", 0), sem("nr", 0), {"tp": flip(chip, z) * CORES + c}
            ).start()
    arrived(gp_v.at[pl.ds(1, tp - 1)], "ar", 0)
    gsum = gp_v[0]
    for j in range(1, tp):
        gsum = gsum + gp_v[j]
    gback_v[0, 0:1, :] = gsum[0:1, :]
    for r in range(1, ep):
        gsum_v[r] = jnp.broadcast_to(gsum[r:r + 1, :], (8, LANES))
        remote(
            gsum_v.at[r], gback_v.at[r], sem("out", 0), sem("br", 0), {"ep": flip(me, r)}
        ).start()
    for s in range(1, len(cuts)):
        kept.append(combine(s, order))
    arrived(gback_v.at[pl.ds(1, ep - 1)], "br", 0)
    res = [jnp.zeros((1, rows), f32), jnp.zeros((1, rows), f32)]
    for r in range(ep):
        col = jnp.sum(jnp.where(square, gback_v[r, 0:1, :], 0.0), axis=1, keepdims=True)
        val = jnp.sum(pk_v[r].astype(f32) * col, axis=0, keepdims=True)
        for k in range(2):
            res[k] = res[k] + jnp.where(rel[k:k + 1, :] == r, val, 0.0)
    dgate_ref[0:1, :] = res[0]
    dgate_ref[1:2, :] = res[1]

    if nz > 1:
        arrived(nr_v.at[pl.ds(1, nz - 1)], "nr", 0)
    norms = nr_v[0].astype(f32)
    for j in range(1, nz):
        norms = norms + nr_v[j].astype(f32)
    gn_ref[...] = norms[0:1, :]
    ln_ref[...] = norms[1:2, :]

    for s in range(len(cuts)):
        lines = slice(marks[s], marks[s + 1])
        at = pl.ds(marks[s], marks[s + 1] - marks[s])
        acc = kept[s]
        if nz > 1:
            arrived(zr_v.at[pl.ds(1, nz - 1), at, :], "zr", s)
        for q in range(1, nz):
            acc = acc + zr_v[q, lines, :].astype(f32)
        dtok_ref[lines, :] = acc.astype(bf16)

    remote_rows = pl.ds(cap, far)
    for s in range(len(cuts)):
        for i, (a, off, w, shared) in enumerate(plan[s]):
            if (s, i) == (0, lone):
                continue
            cols = window(s, i, odd)[1]
            sent(snd_v.at[a, pl.ds(bases[s] - cap, slabs[s]), cols], "out", 0)
            if shared:
                sent(area(s, i, whole(s), odd), "out", 0)
    sent(all_v.at[1, core, remote_rows, :], "out", 0)

    @pl.when(core == CORES - 1)
    def _():
        sent(snd_v.at[0, pl.ds(0, slabs[0]), lone_cols], "out", 0)
        sent(extra_v, "out", 0)
        sent(all_v.at[0, CORES - 1, remote_rows, :], "out", 0)
        sent(all_v.at[0, 0, whole(0), lone_cols], "out", 0)

    @pl.when(core == 0)
    def _():
        sent(all_v.at[0, 0, whole(0), pl.ds(0, lone_off)], "out", 0)
        sent(all_v.at[0, 0, whole(1), :], "out", 0)

    sent(gsnd_v.at[pl.ds(1, ep - 1)], "out", 0)
    sent(ps_v, "out", 0)
    sent(xs_v.at[:, remote_rows, :], "out", 0)
    if nz > 1:
        sent(zs_v.at[pl.ds(1, nz - 1)], "out", 0)
    sent(gp_v.at[pl.ds(1, tp - 1)], "out", 0)
    sent(gsum_v.at[pl.ds(1, ep - 1)], "out", 0)
    sent(ns_v, "out", 0)
    if nz > 1:
        sent(nr_v.at[pl.ds(1, nz - 1)], "out", 0)


def write_out(*refs):
    count = (len(refs) - 1) // 2
    copies = [
        pltpu.make_async_copy(refs[i], refs[count + i], refs[-1].at[i]) for i in range(count)
    ]
    for cp in copies:
        cp.start()
    for cp in copies:
        cp.wait()


def shards(tokens, routes, gates, cotangent, w_glu, w_lin, w_down):
    ep = lax.axis_size("ep")
    tp = lax.axis_size("tp")
    rows, top = routes.shape
    width = tokens.shape[1]
    units = w_glu.shape[2]
    cap = 3 * rows * top // (2 * ep)
    cap = -(-cap // 32) * 32
    slots = ep * cap
    half = width // CORES
    own = width // tp
    nz = tp // CORES
    vm = pl.BlockSpec(memory_space=pltpu.VMEM)
    hbm = pl.BlockSpec(memory_space=pltpu.HBM)
    dma = pltpu.SemaphoreType.DMA
    V = pltpu.VMEM
    out_shape = (
        jax.ShapeDtypeStruct((rows, own), bf16),
        jax.ShapeDtypeStruct((top, rows), f32),
        jax.ShapeDtypeStruct((width, units), f32),
        jax.ShapeDtypeStruct((width, units), f32),
        jax.ShapeDtypeStruct((units, width), f32),
        jax.ShapeDtypeStruct((1, width), f32),
        jax.ShapeDtypeStruct((1, width), f32),
        jax.ShapeDtypeStruct((1, units), f32),
    )
    outs = pl.pallas_call(
        functools.partial(kernel, ep, tp, cap),
        out_shape=out_shape,
        in_specs=[hbm] * 7,
        out_specs=(vm,) * 8,
        scratch_shapes=[
            V((rows, width), bf16),
            V((top, rows), jnp.int32),
            V((top, rows), f32),
            V((rows, width), bf16),
            V((width, units) if units % LANES else (16, LANES), bf16),
            V((width, units) if units % LANES else (16, LANES), bf16),
            V((width, 2 * units), bf16),
            V((units, width), bf16),
            V((rows, slots), bf16),
            V((ep, LANES, rows), bf16),
            V((2, slots - cap, half), bf16),
            V(((ep - 1) * slab_cuts(cap)[0], half // 8), bf16),
            V((2, CORES, slots, half), bf16),
            V((ep, 8, LANES), f32),
            V((ep, 8, LANES), f32),
            V((slots, 2 * units), bf16),
            V((slots, units), bf16),
            V((slots, units), f32),
            V((3 * units, slots), bf16),
            V((nz, slots, own), bf16),
            V((nz, slots, own), bf16),
            V((nz, slots, own), f32),
            V((nz, slots, own), bf16),
            V((nz, slots, own), bf16),
            V((nz, rows, own), bf16),
            V((nz, rows, own), bf16),
            V((tp, ep, LANES), f32),
            V((ep, 8, LANES), f32),
            V((ep, 8, LANES), f32),
            V((2, width), f32),
            V((2, width), f32),
            V((nz, 2, width), bf16),
            dma((len(semaphores(ep, nz, piece_list(half, len(slab_cuts(cap))))),)),
        ],
        compiler_params=pltpu.CompilerParams(
            collective_id=0, has_side_effects=True, vmem_limit_bytes=28 * 1024 * 1024
        ),
    )(*(pltpu.with_memory_space_constraint(x, pltpu.HBM) for x in (
        tokens, routes.T, gates.T, cotangent, w_glu[0], w_lin[0], w_down[0]
    )))
    outs = pl.pallas_call(
        write_out,
        out_shape=out_shape,
        in_specs=[vm] * len(out_shape),
        out_specs=(hbm,) * len(out_shape),
        scratch_shapes=[dma((len(out_shape),))],
        compiler_params=pltpu.CompilerParams(vmem_limit_bytes=28 * 1024 * 1024),
    )(*outs)
    d_tokens, d_gates, gw, lw, dw, gn, ln, dn = outs
    return (d_tokens, d_gates.T, gw[None], lw[None], dw[None], gn, ln, dn)


def solution(mesh):
    in_specs = (
        P("ep", None),
        P("ep", None),
        P("ep", None),
        P("ep", None),
        P("ep", None, "tp"),
        P("ep", None, "tp"),
        P("ep", "tp", None),
    )
    out_specs = (
        P("ep", "tp"),
        P("ep", None),
        P("ep", None, "tp"),
        P("ep", None, "tp"),
        P("ep", "tp", None),
        P("ep", None),
        P("ep", None),
        P("ep", "tp"),
    )
    return jax.shard_map(shards, mesh=mesh, in_specs=in_specs, out_specs=out_specs, check_vma=False)
```
